512 devices in a mesh: ep: 32 (over z, x), tp: 16 (over y, core).
Axes of the slice: x: 4, y: 8, z: 8, core: 2. Of those that a mesh axis runs over, the one named last changes fastest.
Arguments:
- x_in: bfloat16 [4096, 12288], P('tp', 'ep'), may hold values from -6 to 6
- z_in: bfloat16 [4096, 12288], P('tp', 'ep'), may hold values from -6 to 6
- dt_raw: float32 [64, 12288], P('tp', 'ep'), may hold values from -6 to 6
- decay_rate: float32 [64], P('tp'), may hold values from 0 to 1, as said below
- b_in: bfloat16 [256, 12288], P(None, 'ep'), may hold values from -6 to 6
- c_in: bfloat16 [256, 12288], P(None, 'ep'), may hold values from -6 to 6
- conv_x: float32 [4096, 4], P('tp'), may hold values from -3 to 3
- conv_b: float32 [256, 4], replicated, may hold values from -3 to 3
- conv_c: float32 [256, 4], replicated, may hold values from -3 to 3
- head_gain: float32 [4096], P('tp'), may hold values from 0.1 to 1.9
- moe_rows: bfloat16 [5120, 2048], P('ep'), may hold values from -6 to 6
- moe_gain: float32 [2048], replicated, may hold values from 0.1 to 1.9
- routes: int32 [5120, 2], P('ep'), may hold values from 0 to 31, all different within a row; in each aligned block of 160 rows (0 to 159, 160 to 319, ...) at most 20 rows name the same one
- route_logit: float32 [5120, 2], P('ep'), may hold values from -6 to 6
- w_gate: bfloat16 [32, 2048, 5120], P('ep', None, 'tp'), may hold values from -0.125 to 0.125
- w_up: bfloat16 [32, 2048, 5120], P('ep', None, 'tp'), may hold values from -0.125 to 0.125
- w_down: bfloat16 [32, 5120, 2048], P('ep', 'tp'), may hold values from -0.078125 to 0.078125
Outputs:
- mixed: bfloat16 [4096, 12288], P('tp', 'ep')
- moe_out: bfloat16 [2048, 5120], P('tp', 'ep')
The draws below stay inside these ranges and needn't reach their ends.
Inputs may be any that keep to these rules, and one draw needn't show every extreme that they name: `routes`: each row names 2 different experts; among the rows of one index of ep no expert is named more than 20 times, a bound that some block reaches. `decay_rate`: positive rates.
All inputs are finite; a program needn't handle non-finite values.
Results may differ from the reference program's by a relative error of at most 0.018.
Values may be sent and summed in bfloat16 or wider, within the bound.
A program may use at most 64 MiB of HBM per device.

```python
import math
import jax
import jax.numpy as jnp
import numpy as np
from jax import lax

D = 2048
HEADS = 64
HEAD_DIM = 64
GROUPS = 2
NSTATE = 128
KCONV = 4
BLOCK = 128
FF = 5120
TOP = 2
L_DEV = 384
MOE_DEV = 160
SEQLEN = 12288
MTOK = 5120
EXPERTS = 32
CAP = 20
N_EP = 32
N_TP = 16


def draw_decay_rate(key, part):
    order_key, slow_key, fast_key = jax.random.split(jax.random.fold_in(key, 11), 3)
    fast_count = HEADS // 2
    is_fast = jax.random.permutation(order_key, HEADS) < fast_count
    slow_rate = jnp.exp(jax.random.uniform(slow_key, (HEADS,), jnp.float32, math.log(0.05 / SEQLEN), math.log(1.0 / SEQLEN)))
    fast_rate = jnp.exp(jax.random.uniform(fast_key, (HEADS,), jnp.float32, math.log(0.012), math.log(0.04)))
    return jnp.where(is_fast, fast_rate, slow_rate)


def draw_dt_raw(key, part):
    noise_key, span_key, block_key = jax.random.split(jax.random.fold_in(key, 23), 3)
    noise = jnp.clip(0.7 * jax.random.normal(noise_key, (HEADS, SEQLEN), jnp.float32), -4.0, 4.0)
    span_shift = jax.random.uniform(span_key, (HEADS, SEQLEN // L_DEV), jnp.float32, -1.5, 1.5)
    block_shift = jax.random.uniform(block_key, (HEADS, SEQLEN // BLOCK), jnp.float32, -0.5, 0.5)
    return noise + jnp.repeat(span_shift, L_DEV, axis=1) + jnp.repeat(block_shift, BLOCK, axis=1)


def levels(stream_key, extent, pieces, smallest, largest):
    loudness, own = 1.0, jax.random.fold_in(stream_key, 6)
    for axis_at, shards_of in pieces:
        steps = jnp.exp(jax.random.uniform(jax.random.fold_in(own, axis_at), (shards_of,), jnp.float32, smallest / len(pieces), largest / len(pieces)))
        loudness = loudness * jnp.repeat(steps, extent[axis_at] // shards_of).reshape([-1 if axis == axis_at else 1 for axis in range(len(extent))])
    return loudness


def assign_block(stream_key, own, number, rows, amount, top, bound, lean):
    ranking = jax.random.permutation(stream_key, amount)
    crowded, usual = portions_of(amount, rows * top, bound, lean, True), portions_of(amount, rows * top, bound, lean, False)
    places = jnp.arange(amount)

    def named(sizes, rotation):
        used = int((sizes > 0).sum())
        fixed = max(1, used // 4)
        moved = fixed + (places - fixed + rotation * (used - fixed)) % max(1, amount - fixed)
        return jnp.zeros((amount,), jnp.int32).at[ranking[jnp.where(places < fixed, places, moved)]].set(jnp.asarray(sizes, jnp.int32))

    sizes = jnp.where(number % 4 == 0, named(crowded, number // 4), named(usual, number - number // 4 - 1))
    mixed = jax.random.permutation(jax.random.fold_in(own, 3), amount)
    giver, receiver = mixed[0:amount // 2 * 2:2], mixed[1:amount // 2 * 2:2]
    slack = jnp.minimum(sizes[giver] - 1, bound - sizes[receiver]) // 2
    slack = jnp.where((giver == ranking[0]) | (receiver == ranking[0]) | (sizes[receiver] == 0), 0, jnp.maximum(slack, 0))
    moved = jax.random.randint(jax.random.fold_in(own, 4), (amount // 2,), 0, 1 << 20) % (slack + 1)
    sizes = sizes.at[giver].add(-moved).at[receiver].add(moved)
    items = jnp.searchsorted(jnp.cumsum(sizes), jnp.arange(rows * top), side="right").astype(jnp.int32)
    grid = items.reshape(top, rows).T
    grid = grid[jax.random.permutation(jax.random.fold_in(own, 1), rows)]
    rotation = jax.random.randint(jax.random.fold_in(own, 2), (rows, 1), 0, top)
    return jnp.take_along_axis(grid, (jnp.arange(top)[None, :] + rotation) % top, axis=1)


def portions_of(amount, total, most, skew, full):
    loads = [(1 << 20) // math.isqrt(grade ** skew) + 1 for grade in range(1, amount + 1)]
    largest = most if full else min(most, max(-(-total // amount), total * loads[0] // sum(loads)))
    least = 1 if total - largest >= amount - 1 else 0
    given, spare = [largest] + [least] * (amount - 1), total - largest - least * (amount - 1)
    while spare > 0:
        free = [i for i in range(1, amount) if given[i] < largest] or [i for i in range(1, amount) if given[i] < most]
        mass, left = sum([loads[i] for i in free]), spare
        for i in free:
            addition = min(most - given[i], max(1, left * loads[i] // mass), spare)
            given[i] = given[i] + addition
            spare = spare - addition
    return np.array(given)


def gaussian(own_key, dims, width, reach, shards=(), held_as=jnp.bfloat16):
    values = width * jax.random.normal(own_key, dims, jnp.float32)
    if shards:
        values = values * levels(own_key, dims, shards, -0.22, 0.18)
    return jnp.clip(values, -reach, reach).astype(held_as)


def setup_inputs(seed: int = 0) -> dict:
    key_of = jax.random.split(jax.random.key(seed), 18)
    x_in = gaussian(key_of[0], (HEADS * HEAD_DIM, SEQLEN), 1.0, 6.0, ((0, 16), (1, 32)))
    z_in = gaussian(key_of[1], (HEADS * HEAD_DIM, SEQLEN), 1.0, 6.0, ((0, 16), (1, 32)))
    dt_raw = draw_dt_raw(jax.random.fold_in(key_of[17], 71), 0)
    decay_rate = draw_decay_rate(jax.random.fold_in(key_of[17], 71), 0)
    b_in = gaussian(key_of[4], (GROUPS * NSTATE, SEQLEN), 1.0, 6.0, ((1, 32),))
    c_in = gaussian(key_of[5], (GROUPS * NSTATE, SEQLEN), 1.0, 6.0, ((1, 32),))
    conv_x = gaussian(key_of[6], (HEADS * HEAD_DIM, KCONV), KCONV ** -0.5, 3.0, ((0, 16),), jnp.float32)
    conv_b = gaussian(key_of[7], (GROUPS * NSTATE, KCONV), KCONV ** -0.5, 3.0, (), jnp.float32)
    conv_c = gaussian(key_of[8], (GROUPS * NSTATE, KCONV), KCONV ** -0.5, 3.0, (), jnp.float32)
    head_gain = jnp.clip(1.0 + 0.18 * jax.random.normal(key_of[9], (HEADS * HEAD_DIM,), jnp.float32), 0.1, 1.9)
    moe_rows = gaussian(key_of[10], (MTOK, D), 1.0, 6.0, ((0, 32),))
    moe_gain = jnp.clip(1.0 + 0.18 * jax.random.normal(key_of[11], (D,), jnp.float32), 0.1, 1.9)
    routes_keys = jax.random.split(jax.random.fold_in(key_of[12], 1), MTOK // MOE_DEV)
    routes_turns = jax.random.permutation(jax.random.fold_in(key_of[12], 3), MTOK // MOE_DEV)
    routes = jax.vmap(lambda own, number: assign_block(jax.random.fold_in(key_of[12], 2), own, number, MOE_DEV, EXPERTS, TOP, CAP, 2))(routes_keys, routes_turns).reshape((MTOK, TOP))
    route_logit = gaussian(key_of[13], (MTOK, TOP), 1.5, 6.0, ((0, 32),), jnp.float32)
    w_gate = gaussian(key_of[14], (EXPERTS, D, FF), D ** -0.5, 0.125, ((0, 32), (2, 16)))
    w_up = gaussian(key_of[15], (EXPERTS, D, FF), D ** -0.5, 0.125, ((0, 32), (2, 16)))
    w_down = gaussian(key_of[16], (EXPERTS, FF, D), FF ** -0.5, 0.078125, ((0, 32), (1, 16)))
    return dict(x_in=x_in, z_in=z_in, dt_raw=dt_raw, decay_rate=decay_rate, b_in=b_in, c_in=c_in, conv_x=conv_x, conv_b=conv_b, conv_c=conv_c, head_gain=head_gain, moe_rows=moe_rows, moe_gain=moe_gain, routes=routes, route_logit=route_logit, w_gate=w_gate, w_up=w_up, w_down=w_down)


HIGHEST = lax.Precision.HIGHEST
ROW_EPS = 0.1
HEAD_EPS = 1.0

def causal_conv(signal, weight):
    taps = weight.shape[1]
    length = signal.shape[1]
    padded = jnp.pad(signal, ((0, 0), (taps - 1, 0)))
    running = jnp.zeros(signal.shape, jnp.float32)
    for offset in range(taps):
        running = running + weight[:, offset:offset + 1] * padded[:, offset:offset + length]
    return jax.nn.silu(running)

def block_step(state_in, x_block, b_block, c_block, log_block, step_block):
    cum_log = jnp.cumsum(log_block, axis=1)
    seg_log = cum_log[:, :, None] - cum_log[:, None, :]
    causal = jnp.tril(jnp.ones((log_block.shape[1], log_block.shape[1]), bool))
    decay_mask = jnp.exp(jnp.where(causal[None], seg_log, -jnp.inf))
    scores = jnp.einsum('hnt,hns->hts', c_block, b_block, precision=HIGHEST) * decay_mask * step_block[:, None, :]
    inner_term = jnp.einsum('hts,hps->hpt', scores, x_block, precision=HIGHEST)
    carried = jnp.einsum('hnt,hpn->hpt', c_block, state_in, precision=HIGHEST) * jnp.exp(cum_log)[:, None, :]
    tail_weight = jnp.exp(cum_log[:, -1:] - cum_log) * step_block
    fresh_state = jnp.einsum('hps,hns->hpn', x_block * tail_weight[:, None, :], b_block, precision=HIGHEST)
    new_state = jnp.exp(cum_log[:, -1])[:, None, None] * state_in + fresh_state
    return (new_state, inner_term + carried)

def mixer_half(x_in, z_in, dt_raw, decay_rate, b_in, c_in, conv_x, conv_b, conv_c, head_gain):
    x_conv = causal_conv(x_in.astype(jnp.float32), conv_x.astype(jnp.float32)).reshape(HEADS, HEAD_DIM, SEQLEN)
    b_conv = causal_conv(b_in.astype(jnp.float32), conv_b.astype(jnp.float32)).reshape(GROUPS, NSTATE, SEQLEN)
    c_conv = causal_conv(c_in.astype(jnp.float32), conv_c.astype(jnp.float32)).reshape(GROUPS, NSTATE, SEQLEN)
    step_dt = jax.nn.softplus(dt_raw.astype(jnp.float32))
    log_decay = -step_dt * decay_rate.astype(jnp.float32)[:, None]
    block_count = SEQLEN // BLOCK
    per_group = HEADS // GROUPS

    def blocks(tensor):
        return jnp.moveaxis(tensor.reshape(tensor.shape[:-1] + (block_count, BLOCK)), -2, 0)

    def advance(state_in, inputs):
        x_block, b_block, c_block, log_block, step_block = inputs
        return block_step(state_in, x_block, jnp.repeat(b_block, per_group, axis=0), jnp.repeat(c_block, per_group, axis=0), log_block, step_block)
    init_state = jnp.zeros((HEADS, HEAD_DIM, NSTATE), jnp.float32)
    _, block_out = lax.scan(advance, init_state, (blocks(x_conv), blocks(b_conv), blocks(c_conv), blocks(log_decay), blocks(step_dt)))
    y_mixed = jnp.moveaxis(block_out, 0, -2).reshape(HEADS, HEAD_DIM, SEQLEN)
    gated_out = y_mixed * jax.nn.silu(z_in.astype(jnp.float32).reshape(HEADS, HEAD_DIM, SEQLEN))
    head_scale = lax.rsqrt(lax.optimization_barrier(jnp.mean(gated_out * gated_out, axis=1, keepdims=True)) + HEAD_EPS)
    normed_out = gated_out * head_scale * head_gain.astype(jnp.float32).reshape(HEADS, HEAD_DIM, 1)
    return normed_out.reshape(HEADS * HEAD_DIM, SEQLEN).astype(jnp.bfloat16)

def experts_half(moe_rows, moe_gain, routes, route_logit, w_gate, w_up, w_down):
    rows_float = moe_rows.astype(jnp.float32)
    row_scale = lax.rsqrt(lax.optimization_barrier(jnp.mean(rows_float * rows_float, axis=1, keepdims=True)) + ROW_EPS)
    normed = (rows_float * row_scale * moe_gain.astype(jnp.float32)).astype(jnp.bfloat16)
    by_source = routes.reshape(N_EP, MOE_DEV * TOP)
    hit_table = (by_source[:, :, None] == jnp.arange(EXPERTS, dtype=jnp.int32)).astype(jnp.int32)
    slot_rank = lax.optimization_barrier(jnp.sum((jnp.cumsum(hit_table, axis=1) - hit_table) * hit_table, axis=2))
    slot_index = (jnp.arange(N_EP, dtype=jnp.int32)[:, None] * CAP + slot_rank).reshape(-1).astype(jnp.int32)
    expert_index = routes.reshape(-1).astype(jnp.int32)
    token_index = (jnp.arange(MTOK * TOP, dtype=jnp.int32) // TOP).astype(jnp.int32)
    buffer = jnp.zeros((EXPERTS, N_EP * CAP, D), jnp.bfloat16).at[expert_index, slot_index].set(normed[token_index])
    block_width = FF // N_TP

    def run_expert(inputs):
        rows_in, gate_weight, up_weight, down_weight = inputs
        gate_act = jnp.dot(rows_in, gate_weight, preferred_element_type=jnp.float32)
        up_act = jnp.dot(rows_in, up_weight, preferred_element_type=jnp.float32)
        hidden = (jax.nn.silu(gate_act) * up_act).astype(jnp.bfloat16)
        running = jnp.zeros((rows_in.shape[0], D), jnp.float32)
        for part_index in range(N_TP):
            lower = part_index * block_width
            piece_sum = jnp.dot(hidden[:, lower:lower + block_width], down_weight[lower:lower + block_width], preferred_element_type=jnp.float32)
            running = running + lax.optimization_barrier(piece_sum.astype(jnp.bfloat16)).astype(jnp.float32)
        return running.astype(jnp.bfloat16)
    results = lax.map(run_expert, (buffer, w_gate, w_up, w_down))
    picked = results[expert_index, slot_index].astype(jnp.float32).reshape(MTOK, TOP, D)
    weight = jax.nn.sigmoid(route_logit - route_logit[:, ::-1])
    combined = lax.optimization_barrier(jnp.sum(picked * weight[:, :, None], axis=1))
    return combined.T.astype(jnp.bfloat16)

def reference(x_in, z_in, dt_raw, decay_rate, b_in, c_in, conv_x, conv_b, conv_c, head_gain, moe_rows, moe_gain, routes, route_logit, w_gate, w_up, w_down):
    mixed = mixer_half(x_in, z_in, dt_raw, decay_rate, b_in, c_in, conv_x, conv_b, conv_c, head_gain)
    moe_out = experts_half(moe_rows, moe_gain, routes, route_logit, w_gate, w_up, w_down)
    return (mixed, moe_out)
```

```python
import functools

import jax
import jax.numpy as jnp
from jax import lax
from jax.experimental import pallas as pl
from jax.experimental.pallas import tpu as pltpu
from jax.sharding import PartitionSpec as P

F32 = jnp.float32
BF16 = jnp.bfloat16
MESH = pl.DeviceIdType.MESH
HIGHEST = lax.Precision.HIGHEST
GROUPS = 2
NSTATE = 128
LANES = 128
QUAD = 4
ROW_EPS = 0.1
HEAD_EPS = 1.0


def mm(a, b, dims=(((1,), (0,)), ((), ()))):
    return lax.dot_general(a, b, dims, preferred_element_type=F32)


def kernel_body(
    cfg,
    x_hbm, z_hbm, dt_ref, rate_ref, b_hbm, c_hbm, tapx_ref, tapb_ref, tapc_ref, hgain_ref,
    rows_hbm, mgain_ref, routes_ref, logit_ref, wg_hbm, wu_hbm, wd_hbm,
    mixed_ref, moe_ref,
    x_v, z_v, b_v, c_v, rows_v, wg_v, wu_v, wd_v, halo, pick, outbox, xall,
    gate_acc, up_acc, hid, part, sib, tosend, arrived, rout, rin,
    xs_v, bc_v, cc_v, cum_v, colv, yloc, sout, sin, hout, hin,
    load_sem, halo_send, halo_recv, disp_send, disp_recv, st_send, st_recv, hb_send, hb_recv,
    ag_send, ag_recv, d2_send, d2_recv, ps_send, ps_recv, rs_send, rs_recv, rt_send, rt_recv,
):
    EP, TP, CAP, L, HH = cfg["EP"], cfg["TP"], cfg["CAP"], cfg["L"], cfg["HH"]
    NY = TP // 2
    UC = CAP // QUAD
    ROWS = EP * CAP
    HALF = ROWS // QUAD // 2
    tokens = rows_v.shape[0]
    VR = x_v.shape[0]
    HD = VR // HH
    NB = L // LANES
    U = VR // EP
    UR = sout.shape[1]
    ep, tp = lax.axis_index("ep"), lax.axis_index("tp")
    y, core = lax.div(tp, 2), lax.rem(tp, 2)
    other = 1 - core
    group = lax.div(tp, TP // GROUPS)

    def to_ep(d):
        return {"ep": lax.rem(ep + d, EP), "tp": tp}

    def to_y(s):
        return {"ep": ep, "tp": lax.rem(y + s + NY, NY) * 2 + core}

    sibling = {"ep": ep, "tp": y * 2 + other}

    def rcopy(src, dst, ssem, rsem, dev):
        return pltpu.make_async_remote_copy(
            src_ref=src, dst_ref=dst, send_sem=ssem, recv_sem=rsem, device_id=dev, device_id_type=MESH
        )

    def flat(block):
        return block.reshape(block.shape[0] * QUAD, LANES)

    def put(ref, value):
        ref[...] = value.reshape(value.shape[0] // QUAD, QUAD, LANES)

    def wait_bytes(ref, sem):
        pltpu.make_async_copy(ref, ref, sem).wait()

    gsel = pl.ds(pl.multiple_of(group * NSTATE, NSTATE), NSTATE)
    loads = [
        pltpu.make_async_copy(src, dst, load_sem.at[i])
        for i, (src, dst) in enumerate(
            (
                (rows_hbm, rows_v), (x_hbm, x_v), (b_hbm.at[gsel, :], b_v), (c_hbm.at[gsel, :], c_v),
                (wg_hbm.at[0], wg_v), (wu_hbm.at[0], wu_v), (wd_hbm.at[0], wd_v), (z_hbm, z_v),
            )
        )
    ]
    for load in loads:
        load.start()

    barrier = pltpu.get_barrier_semaphore()

    @pl.loop(1, EP)
    def _(d):
        pl.semaphore_signal(barrier, inc=1, device_id=to_ep(d), device_id_type=MESH)

    for dev in (to_y(1), to_y(-1), sibling):
        pl.semaphore_signal(barrier, inc=1, device_id=dev, device_id_type=MESH)

    routes = routes_ref[...]
    lane_e = lax.broadcasted_iota(jnp.int32, (tokens, EP), 1)
    hits = [(routes[:, k : k + 1] == lane_e).astype(F32) for k in range(2)]
    below = (
        lax.broadcasted_iota(jnp.int32, (tokens, tokens), 0)
        > lax.broadcasted_iota(jnp.int32, (tokens, tokens), 1)
    ).astype(BF16)
    ahead = mm(below, (hits[0] + hits[1]).astype(BF16))
    lane_s = lax.broadcasted_iota(jnp.int32, (tokens, ROWS), 1)
    onehot = None
    for k in range(2):
        rank = jnp.sum(ahead * hits[k], axis=1, keepdims=True).astype(jnp.int32)
        slot = routes[:, k : k + 1] * CAP + rank
        hot = (lane_s == slot).astype(F32)
        pick[k] = hot.astype(BF16)
        onehot = hot if onehot is None else onehot + hot

    loads[0].wait()
    rows_f = rows_v[...].astype(F32)
    row_scale = lax.rsqrt(jnp.mean(rows_f * rows_f, axis=1, keepdims=True) + ROW_EPS)
    own_cols = rows_v[:, pl.ds(pl.multiple_of(tp * LANES, LANES), LANES)].astype(F32)
    normed = (own_cols * row_scale * mgain_ref[pl.ds(tp, 1), :]).astype(BF16)
    packed = mm(onehot.astype(BF16), normed, (((0,), (0,)), ((), ()))).astype(BF16)
    put(outbox, packed)

    for i in (1, 2, 3):
        loads[i].wait()
    pl.semaphore_wait(barrier, EP - 1 + 3)

    @pl.loop(1, EP)
    def _(d):
        tgt = lax.rem(ep + d, EP)
        rcopy(
            outbox.at[pl.ds(tgt * UC, UC)], xall.at[tp, pl.ds(ep * UC, UC)], disp_send, disp_recv, to_ep(d)
        ).start()

    last = pl.ds(L - LANES, LANES)
    halos = [
        rcopy(x_v.at[:, last], halo.at[pl.ds(0, VR)], halo_send.at[0], halo_recv.at[0], to_ep(1)),
        rcopy(b_v.at[:, last], halo.at[pl.ds(VR, NSTATE)], halo_send.at[1], halo_recv.at[1], to_ep(1)),
        rcopy(
            c_v.at[:, last], halo.at[pl.ds(VR + NSTATE, NSTATE)], halo_send.at[2], halo_recv.at[2], to_ep(1)
        ),
    ]
    for h in halos:
        h.start()
    xall[tp, pl.ds(ep * UC, UC)] = outbox[pl.ds(ep * UC, UC)]

    dt = dt_ref[...]
    step = jnp.maximum(dt, 0.0) + jnp.log1p(jnp.exp(-jnp.abs(dt)))
    head_row = lax.broadcasted_iota(jnp.int32, (HH, L), 0)
    rate = jnp.zeros((HH, L), F32)
    for h in range(HH):
        rate = jnp.where(head_row == h, rate_ref[h], rate)
    logd = -step * rate
    upper = (
        lax.broadcasted_iota(jnp.int32, (LANES, LANES), 0)
        <= lax.broadcasted_iota(jnp.int32, (LANES, LANES), 1)
    ).astype(F32)
    pieces, carry = [], jnp.zeros((HH, 1), F32)
    for k in range(NB):
        piece = (
            jnp.dot(
                logd[:, k * LANES : (k + 1) * LANES], upper, precision=HIGHEST, preferred_element_type=F32
            )
            + carry
        )
        carry = piece[:, LANES - 1 : LANES]
        pieces.append(piece)
    cum = jnp.concatenate(pieces, axis=1)
    total = carry
    cum_v[pl.ds(0, HH), :] = cum
    tall = jnp.concatenate([cum, jnp.zeros((8 - HH, L), F32)], axis=0)
    colv[...] = jnp.transpose(tall)

    for h in halos:
        h.wait_recv()
    started = (ep > 0).astype(F32)

    def conv(cur, rim, taps):
        joined = jnp.concatenate([rim.astype(F32) * started, cur.astype(F32)], axis=1)
        out = taps[:, 3:4] * joined[:, LANES:]
        for k in range(3):
            out = out + taps[:, k : k + 1] * pltpu.roll(joined, 3 - k, 1)[:, LANES:]
        return out * jax.nn.sigmoid(out)

    b_conv = conv(b_v[...], halo[pl.ds(VR, NSTATE), :], tapb_ref[gsel, :]).astype(BF16)
    bc_v[...] = b_conv
    tail = jnp.exp(total - cum)
    for h in range(HH):
        rows_h = pl.ds(h * HD, HD)
        xc = conv(x_v[rows_h, :], halo[rows_h, :], tapx_ref[rows_h, :])
        xs = xc * step[h : h + 1, :]
        xs_v[rows_h, :] = xs.astype(BF16)
        yloc[rows_h, :] = xs * tail[h : h + 1, :]
    state = mm(yloc[...].astype(BF16), b_conv, (((1,), (1,)), ((), ())))

    hi = total.astype(BF16).astype(F32)
    mid = (total - hi).astype(BF16).astype(F32)
    low = total - hi - mid
    r8 = lax.broadcasted_iota(jnp.int32, (8, LANES), 0)
    decays = []
    for u in range(EP):
        h = u * U // HD
        decays.append(
            jnp.where(
                r8 == 0,
                hi[h : h + 1],
                jnp.where(r8 == 1, mid[h : h + 1], jnp.where(r8 == 2, low[h : h + 1], 0.0)),
            )
        )
    for u in range(EP):
        extra = [state[u * U : (u + 1) * U], decays[u]]
        if UR > U + 8:
            extra.append(jnp.zeros((UR - U - 8, LANES), F32))
        sout[u] = jnp.concatenate(extra, axis=0).astype(BF16)

    @pl.loop(1, EP)
    def _(d):
        tgt = lax.rem(ep + d, EP)
        rcopy(sout.at[tgt], sin.at[ep], st_send, st_recv, to_ep(d)).start()

    sin[ep] = sout[ep]

    streams = [(0, 1, NY // 2), (1, -1, NY // 2), (0, -1, NY // 2 - 1), (1, 1, NY // 2 - 1)]

    def lane(o, c):
        return lax.rem(y + o + NY, NY) * 2 + c

    def chunk(c):
        return pl.ds(c * HALF, HALF)

    def ring(k, i):
        c, s, _ = streams[k]
        t = lane(-s * i, core)
        blk = xall.at[t, chunk(c)]
        return rcopy(blk, blk, ag_send, ag_recv.at[k, i], to_y(s))

    def ring_recv(k, i):
        c, s, _ = streams[k]
        t = lane(-s * (i + 1), core)
        blk = xall.at[t, chunk(c)]
        return rcopy(blk, blk, ag_send, ag_recv.at[k, i], to_y(s))

    def cross(o, c):
        blk = xall.at[lane(o, core), chunk(c)]
        return rcopy(blk, blk, d2_send, d2_recv.at[o % NY, c], sibling)

    def cross_recv(o, c):
        blk = xall.at[lane(o, other), chunk(c)]
        return rcopy(blk, blk, d2_send, d2_recv.at[o % NY, c], sibling)

    def expand(o, first=False):
        for c in range(2):
            cross_recv(o, c).wait_recv()
        yy = lax.rem(y + o + NY, NY)
        rows = jnp.concatenate(
            [flat(xall[2 * yy]), flat(xall[2 * yy + 1])], axis=1
        )
        ks = pl.ds(pl.multiple_of(yy * 2 * LANES, 2 * LANES), 2 * LANES)
        for acc, w in ((gate_acc, wg_v), (up_acc, wu_v)):
            prod = mm(rows, w[ks, :])
            if first:
                acc[...] = prod
            else:
                acc[...] += prod

    wait_bytes(outbox.at[pl.ds(0, (EP - 1) * UC)], disp_recv)
    for k in range(4):
        if streams[k][2] > 0:
            ring(k, 0).start()
    for c in range(2):
        cross(0, c).start()
    loads[4].wait()
    loads[5].wait()

    def local_part():
        c_conv = conv(c_v[...], halo[pl.ds(VR + NSTATE, NSTATE), :], tapc_ref[gsel, :]).astype(BF16)
        cc_v[...] = c_conv
        gram = mm(bc_v[...], c_conv, (((0,), (0,)), ((), ())))
        diag = lax.broadcasted_iota(jnp.int32, (LANES, LANES), 0) <= lax.broadcasted_iota(
            jnp.int32, (LANES, LANES), 1
        )
        for h in range(HH):
            for j in range(NB):
                at = cum_v[h : h + 1, j * LANES : (j + 1) * LANES]
                pieces = []
                for i in range(j + 1):
                    gap = at - colv[i * LANES : (i + 1) * LANES, h : h + 1]
                    if i == j:
                        gap = jnp.where(diag, gap, -jnp.inf)
                    g = gram[i * LANES : (i + 1) * LANES, j * LANES : (j + 1) * LANES]
                    pieces.append((g * jnp.exp(gap)).astype(BF16))
                weights = jnp.concatenate(pieces, axis=0) if j else pieces[0]
                rows_h = pl.ds(h * HD, HD)
                yloc[rows_h, j * LANES : (j + 1) * LANES] = mm(
                    xs_v[rows_h, : (j + 1) * LANES], weights
                )

    def prefix_part():
        wait_bytes(sout.at[pl.ds(0, EP - 1)], st_recv)
        held = jnp.zeros((U, LANES), F32)
        for e in range(EP):
            hout[e] = held
            blk = sin[e].astype(F32)
            keep = jnp.exp(blk[U : U + 1] + blk[U + 1 : U + 2] + blk[U + 2 : U + 3])
            held = keep * held + blk[:U]

        @pl.loop(1, EP)
        def _(d):
            tgt = lax.rem(ep + d, EP)
            rcopy(hout.at[tgt], hin.at[ep], hb_send, hb_recv, to_ep(d)).start()

        hin[ep] = hout[ep]

    def final_part():
        loads[7].wait()
        wait_bytes(hout.at[pl.ds(0, EP - 1)], hb_recv)
        before = hin[...].reshape(VR, LANES).astype(BF16)
        tall = jnp.concatenate([hgain_ref[...], jnp.zeros((8 - VR // LANES, LANES), F32)], axis=0)
        gains = jnp.transpose(tall)
        for h in range(HH):
            rows_h = pl.ds(h * HD, HD)
            carried = mm(before[h * HD : (h + 1) * HD], cc_v[...]) * jnp.exp(cum_v[h : h + 1, :])
            z = z_v[rows_h, :].astype(F32)
            gated = (yloc[rows_h, :] + carried) * (z * jax.nn.sigmoid(z))
            scale = lax.rsqrt(jnp.mean(gated * gated, axis=0, keepdims=True) + HEAD_EPS)
            lo = h * HD % LANES
            gain = gains[lo : lo + HD, h * HD // LANES : h * HD // LANES + 1]
            mixed_ref[rows_h, :] = (gated * scale * gain).astype(BF16)

    fill_gather = {0: local_part, 1: prefix_part}
    for i in range(NY // 2):
        if i in fill_gather:
            fill_gather[i]()
        expand(i, first=(i == 0))
        if i:
            expand(-i)
        for k in range(4):
            c, s, n = streams[k]
            if i < n:
                ring_recv(k, i).wait_recv()
                if i + 1 < n:
                    ring(k, i + 1).start()
                cross(-s * (i + 1), c).start()
    expand(NY // 2)

    gate = gate_acc[...]
    hid[...] = (gate * jax.nn.sigmoid(gate) * up_acc[...]).astype(BF16)

    loads[6].wait()

    def swap(o):
        return rcopy(part.at[o % NY, other], sib.at[o % NY], ps_send, ps_recv.at[o % NY], sibling)

    def project(o):
        yy = lax.rem(y + o + NY, NY)
        cols = pl.ds(pl.multiple_of(yy * 2 * LANES, 2 * LANES), 2 * LANES)
        prod = mm(hid[...], wd_v[:, cols]).astype(BF16)
        put(part.at[o % NY, 0], prod[:, :LANES])
        put(part.at[o % NY, 1], prod[:, LANES:])
        swap(o).start()

    swapped = set()

    def pair_sum(o, c):
        if o % NY not in swapped:
            swap(o).wait_recv()
            swapped.add(o % NY)
        mine = flat(part[o % NY, core, chunk(c)]).astype(F32)
        return mine + flat(sib[o % NY, chunk(c)]).astype(F32)

    slots, count = {}, 0
    for k in range(4):
        for i in range(streams[k][2]):
            slots[k, i] = count
            count += 1

    def push(k, i):
        j = slots[k, i]
        return rcopy(tosend.at[j], arrived.at[j], rs_send, rs_recv.at[j], to_y(streams[k][1]))

    def came(k, i):
        push(k, i).wait_recv()
        return flat(arrived[slots[k, i]]).astype(F32)

    reach = NY // 2
    project(reach)
    if reach > 1:
        project(reach - 1)
        project(1 - reach)
    fill_scatter = {1: final_part}
    for i in range(reach):
        for k in range(4):
            c, s, n = streams[k]
            if i < n:
                value = pair_sum(s * (n - i), c)
                if i:
                    value = value + came(k, i - 1)
                put(tosend.at[slots[k, i]], value.astype(BF16))
                push(k, i).start()
        left = reach - 2 - i
        if left >= 0:
            project(left)
            if left:
                project(-left)
        if i in fill_scatter:
            fill_scatter[i]()
    if reach == 1:
        project(0)
    for c in range(2):
        value = pair_sum(0, c)
        for k in range(4):
            if streams[k][0] == c and streams[k][2] > 0:
                value = value + came(k, streams[k][2] - 1)
        put(rout.at[chunk(c)], value.astype(BF16))

    @pl.loop(1, EP)
    def _(d):
        tgt = lax.rem(ep + d, EP)
        rcopy(
            rout.at[pl.ds(tgt * UC, UC)], rin.at[pl.ds(ep * UC, UC)], rt_send, rt_recv, to_ep(d)
        ).start()

    rin[pl.ds(ep * UC, UC)] = rout[pl.ds(ep * UC, UC)]
    logit = logit_ref[...]
    w0 = jax.nn.sigmoid(logit[:, 0:1] - logit[:, 1:2])
    w1 = jax.nn.sigmoid(logit[:, 1:2] - logit[:, 0:1])

    wait_bytes(outbox.at[pl.ds(0, (EP - 1) * UC)], disp_send)
    for h in halos:
        h.wait_send()
    wait_bytes(sout.at[pl.ds(0, EP - 1)], st_send)
    wait_bytes(hout.at[pl.ds(0, EP - 1)], hb_send)
    wait_bytes(xall.at[pl.ds(0, NY - 1)], ag_send)
    wait_bytes(xall.at[pl.ds(0, NY)], d2_send)
    wait_bytes(sib, ps_send)
    wait_bytes(tosend, rs_send)

    wait_bytes(rout.at[pl.ds(0, (EP - 1) * UC)], rt_recv)
    back = flat(rin[...])
    mixed_rows = mm(pick[0], back) * w0 + mm(pick[1], back) * w1
    moe_ref[...] = jnp.transpose(mixed_rows).astype(BF16)
    wait_bytes(rout.at[pl.ds(0, (EP - 1) * UC)], rt_send)


def on_device(EP, TP, *args):
    (x_in, z_in, dt_raw, decay_rate, b_in, c_in, conv_x, conv_b, conv_c, head_gain,
     moe_rows, moe_gain, routes, route_logit, w_gate, w_up, w_down) = args
    tokens, features = moe_rows.shape
    CAP = 2 * tokens * routes.shape[1] // EP
    VR, L = x_in.shape
    HH = dt_raw.shape[0]
    FD = w_gate.shape[2]
    NY = TP // 2
    ROWS = EP * CAP
    U = VR // EP
    UR = -(-(U + 8) // 16) * 16
    cfg = dict(EP=EP, TP=TP, CAP=CAP, L=L, HH=HH)
    any_, vmem, smem = (pl.BlockSpec(memory_space=m) for m in (pl.ANY, pltpu.VMEM, pltpu.SMEM))
    dma = pltpu.SemaphoreType.DMA
    units = (ROWS // QUAD, QUAD, LANES)
    half = (ROWS // QUAD // 2, QUAD, LANES)
    hops = 2 * (NY // 2) + 2 * (NY // 2 - 1)
    scratch = [
        pltpu.VMEM((VR, L), BF16), pltpu.VMEM((VR, L), BF16),
        pltpu.VMEM((NSTATE, L), BF16), pltpu.VMEM((NSTATE, L), BF16),
        pltpu.VMEM((tokens, features), BF16),
        pltpu.VMEM((features, FD), BF16), pltpu.VMEM((features, FD), BF16), pltpu.VMEM((FD, features), BF16),
        pltpu.VMEM((VR + 2 * NSTATE, LANES), BF16),
        pltpu.VMEM((2, tokens, ROWS), BF16),
        pltpu.VMEM(units, BF16), pltpu.VMEM((TP,) + units, BF16),
        pltpu.VMEM((ROWS, FD), F32), pltpu.VMEM((ROWS, FD), F32), pltpu.VMEM((ROWS, FD), BF16),
        pltpu.VMEM((NY, 2) + units, BF16), pltpu.VMEM((NY,) + units, BF16),
        pltpu.VMEM((hops,) + half, BF16), pltpu.VMEM((hops,) + half, BF16),
        pltpu.VMEM(units, BF16), pltpu.VMEM(units, BF16),
        pltpu.VMEM((VR, L), BF16), pltpu.VMEM((NSTATE, L), BF16), pltpu.VMEM((NSTATE, L), BF16),
        pltpu.VMEM((8, L), F32), pltpu.VMEM((L, 8), F32), pltpu.VMEM((VR, L), F32),
        pltpu.VMEM((EP, UR, LANES), BF16), pltpu.VMEM((EP, UR, LANES), BF16),
        pltpu.VMEM((EP, U, LANES), F32), pltpu.VMEM((EP, U, LANES), F32),
        dma((8,)), dma((3,)), dma((3,)), dma, dma, dma, dma, dma, dma,
        dma, dma((4, NY // 2)), dma, dma((NY, 2)), dma, dma((NY,)), dma, dma((hops,)), dma, dma,
    ]
    return pl.pallas_call(
        functools.partial(kernel_body, cfg),
        name="mixer_and_experts",
        out_shape=(
            jax.ShapeDtypeStruct((VR, L), BF16),
            jax.ShapeDtypeStruct((features // TP, tokens), BF16),
        ),
        in_specs=[
            any_, any_, vmem, smem, any_, any_, vmem, vmem, vmem, vmem,
            any_, vmem, vmem, vmem, any_, any_, any_,
        ],
        out_specs=(vmem, vmem),
        scratch_shapes=scratch,
        compiler_params=pltpu.CompilerParams(
            collective_id=0, has_side_effects=True, vmem_limit_bytes=60 * 1024 * 1024
        ),
    )(
        x_in, z_in, dt_raw, decay_rate, b_in, c_in, conv_x, conv_b, conv_c,
        head_gain.reshape(VR // LANES, LANES), moe_rows, moe_gain.reshape(TP, features // TP),
        routes, route_logit, w_gate, w_up, w_down,
    )


def solution(mesh):
    EP, TP = mesh.shape["ep"], mesh.shape["tp"]
    in_specs = (
        P("tp", "ep"), P("tp", "ep"), P("tp", "ep"), P("tp"), P(None, "ep"), P(None, "ep"),
        P("tp", None), P(), P(), P("tp"), P("ep", None), P(), P("ep", None), P("ep", None),
        P("ep", None, "tp"), P("ep", None, "tp"), P("ep", "tp", None),
    )
    return jax.shard_map(
        functools.partial(on_device, EP, TP),
        mesh=mesh,
        in_specs=in_specs,
        out_specs=(P("tp", "ep"), P("tp", "ep")),
        check_vma=False,
    )
```

```python
import functools

import jax
import jax.numpy as jnp
from jax import lax
from jax.experimental import pallas as pl
from jax.experimental.pallas import tpu as pltpu
from jax.sharding import PartitionSpec as P

F32 = jnp.float32
BF16 = jnp.bfloat16
MESH = pl.DeviceIdType.MESH
HIGHEST = lax.Precision.HIGHEST
GROUPS = 2
NSTATE = 128
LANES = 128
QUAD = 4
ROW_EPS = 0.1
HEAD_EPS = 1.0


def mm(a, b, dims=(((1,), (0,)), ((), ()))):
    return lax.dot_general(a, b, dims, preferred_element_type=F32)


def kernel_body(
    cfg,
    x_hbm, z_hbm, dt_hbm, rate_hbm, b_hbm, c_hbm, tapx_hbm, tapb_hbm, tapc_hbm, hgain_hbm,
    rows_hbm, mgain_hbm, routes_hbm, logit_hbm, wg_hbm, wu_hbm, wd_hbm,
    mixed_hbm, moe_hbm,
    dt_ref, rate_ref, tapx_ref, tapb_ref, tapc_ref, hgain_ref, mgain_ref, routes_ref, logit_ref,
    mixed_ref, moe_ref,
    x_v, z_v, b_v, c_v, rows_v, wg_v, wu_v, wd_v, halo, pick, outbox, xall,
    gate_acc, up_acc, hid, part, sib, tosend, arrived, rout, rin,
    xs_v, bc_v, cc_v, cum_v, colv, yloc, sout, sin, hout, hin,
    load_sem, store_sem, halo_send, halo_recv, disp_send, disp_recv, st_send, st_recv, hb_send, hb_recv,
    ag_send, ag_recv, d2_send, d2_recv, ps_send, ps_recv, rs_send, rs_recv, rt_send, rt_recv,
):
    EP, TP, CAP, L, HH = cfg["EP"], cfg["TP"], cfg["CAP"], cfg["L"], cfg["HH"]
    NY = TP // 2
    UC = CAP // QUAD
    ROWS = EP * CAP
    HALF = ROWS // QUAD // 2
    tokens = rows_v.shape[0]
    VR = x_v.shape[0]
    HD = VR // HH
    NB = L // LANES
    U = VR // EP
    UR = sout.shape[1]
    ep, tp = lax.axis_index("ep"), lax.axis_index("tp")
    y, core = lax.div(tp, 2), lax.rem(tp, 2)
    other = 1 - core
    group = lax.div(tp, TP // GROUPS)

    def to_ep(d):
        return {"ep": lax.rem(ep + d, EP), "tp": tp}

    def to_y(s):
        return {"ep": ep, "tp": lax.rem(y + s + NY, NY) * 2 + core}

    sibling = {"ep": ep, "tp": y * 2 + other}

    def rcopy(src, dst, ssem, rsem, dev):
        return pltpu.make_async_remote_copy(
            src_ref=src, dst_ref=dst, send_sem=ssem, recv_sem=rsem, device_id=dev, device_id_type=MESH
        )

    def flat(block):
        return block.reshape(block.shape[0] * QUAD, LANES)

    def put(ref, value):
        ref[...] = value.reshape(value.shape[0] // QUAD, QUAD, LANES)

    def wait_bytes(ref, sem):
        pltpu.make_async_copy(ref, ref, sem).wait()

    barrier = pltpu.get_barrier_semaphore()

    @pl.loop(1, EP)
    def _(d):
        pl.semaphore_signal(barrier, inc=1, device_id=to_ep(d), device_id_type=MESH)

    for dev in (to_y(1), to_y(-1), sibling):
        pl.semaphore_signal(barrier, inc=1, device_id=dev, device_id_type=MESH)

    gsel = pl.ds(pl.multiple_of(group * NSTATE, NSTATE), NSTATE)
    loads = {}
    for i, (name, src, dst) in enumerate(
        (
            ("routes", routes_hbm, routes_ref), ("rows", rows_hbm, rows_v), ("mgain", mgain_hbm, mgain_ref),
            ("logit", logit_hbm, logit_ref), ("dt", dt_hbm, dt_ref), ("rate", rate_hbm, rate_ref),
            ("x", x_hbm, x_v), ("b", b_hbm.at[gsel, :], b_v), ("c", c_hbm.at[gsel, :], c_v),
            ("tapx", tapx_hbm, tapx_ref), ("tapb", tapb_hbm, tapb_ref), ("tapc", tapc_hbm, tapc_ref),
            ("hgain", hgain_hbm, hgain_ref),
            ("wg", wg_hbm.at[0], wg_v), ("wu", wu_hbm.at[0], wu_v), ("wd", wd_hbm.at[0], wd_v),
            ("z", z_hbm, z_v),
        )
    ):
        loads[name] = pltpu.make_async_copy(src, dst, load_sem.at[i])
        loads[name].start()

    def ready(*names):
        for name in names:
            loads[name].wait()

    ready("routes")
    routes = routes_ref[...]
    row_e = lax.broadcasted_iota(jnp.int32, (EP, tokens), 0)
    hits = [(routes[k : k + 1, :] == row_e).astype(F32) for k in range(2)]
    before = (
        lax.broadcasted_iota(jnp.int32, (tokens, tokens), 0)
        < lax.broadcasted_iota(jnp.int32, (tokens, tokens), 1)
    ).astype(BF16)
    ahead = mm((hits[0] + hits[1]).astype(BF16), before)
    row_s = lax.broadcasted_iota(jnp.int32, (ROWS, tokens), 0)
    hots = []
    for k in range(2):
        rank = jnp.sum(ahead * hits[k], axis=0, keepdims=True).astype(jnp.int32)
        hots.append(row_s == routes[k : k + 1, :] * CAP + rank)
    onehot = (hots[0] | hots[1]).astype(F32).astype(BF16)

    ready("rows", "mgain")
    rows_f = rows_v[...].astype(F32)
    row_scale = lax.rsqrt(jnp.mean(rows_f * rows_f, axis=1, keepdims=True) + ROW_EPS)
    own_cols = rows_v[:, pl.ds(pl.multiple_of(tp * LANES, LANES), LANES)].astype(F32)
    normed = (own_cols * row_scale * mgain_ref[pl.ds(tp, 1), :]).astype(BF16)
    packed = mm(onehot, normed).astype(BF16)
    put(outbox, packed)

    pl.semaphore_wait(barrier, EP - 1 + 3)

    @pl.loop(1, EP)
    def _(d):
        tgt = lax.rem(ep + d, EP)
        rcopy(
            outbox.at[pl.ds(tgt * UC, UC)], xall.at[tp, pl.ds(ep * UC, UC)], disp_send, disp_recv, to_ep(d)
        ).start()

    xall[tp, pl.ds(ep * UC, UC)] = outbox[pl.ds(ep * UC, UC)]

    ready("logit", "dt", "rate")
    logit = logit_ref[...]
    share = jax.nn.sigmoid(logit[0:1, :] - logit[1:2, :])
    weighted = jnp.where(hots[0], share, jnp.where(hots[1], jax.nn.sigmoid(logit[1:2, :] - logit[0:1, :]), 0.0))
    weighted = jnp.transpose(weighted)
    coarse = weighted.astype(BF16)
    pick[0] = coarse
    pick[1] = (weighted - coarse.astype(F32)).astype(BF16)

    dt = dt_ref[...]
    step = jnp.maximum(dt, 0.0) + jnp.log1p(jnp.exp(-jnp.abs(dt)))
    eye = lax.broadcasted_iota(jnp.int32, (HH, HH), 0) == lax.broadcasted_iota(jnp.int32, (HH, HH), 1)
    rate = jnp.sum(jnp.where(eye, rate_ref[...], 0.0), axis=1, keepdims=True)
    logd = -step * rate
    upper = (
        lax.broadcasted_iota(jnp.int32, (LANES, LANES), 0)
        <= lax.broadcasted_iota(jnp.int32, (LANES, LANES), 1)
    ).astype(F32)
    pieces, carry = [], jnp.zeros((HH, 1), F32)
    for k in range(NB):
        piece = (
            jnp.dot(
                logd[:, k * LANES : (k + 1) * LANES], upper, precision=HIGHEST, preferred_element_type=F32
            )
            + carry
        )
        carry = piece[:, LANES - 1 : LANES]
        pieces.append(piece)
    cum = jnp.concatenate(pieces, axis=1)
    total = carry
    cum_v[pl.ds(0, HH), :] = cum
    tall = jnp.concatenate([cum, jnp.zeros((8 - HH, L), F32)], axis=0)
    colv[...] = jnp.transpose(tall)

    streams = [(0, 1, NY // 2), (1, -1, NY // 2), (0, -1, NY // 2 - 1), (1, 1, NY // 2 - 1)]

    def lane(o, c):
        return lax.rem(y + o + NY, NY) * 2 + c

    def chunk(c):
        return pl.ds(c * HALF, HALF)

    def ring(k, i):
        c, s, _ = streams[k]
        t = lane(-s * i, core)
        blk = xall.at[t, chunk(c)]
        return rcopy(blk, blk, ag_send, ag_recv.at[k, i], to_y(s))

    def ring_recv(k, i):
        c, s, _ = streams[k]
        t = lane(-s * (i + 1), core)
        blk = xall.at[t, chunk(c)]
        return rcopy(blk, blk, ag_send, ag_recv.at[k, i], to_y(s))

    def cross(o, c):
        blk = xall.at[lane(o, core), chunk(c)]
        return rcopy(blk, blk, d2_send, d2_recv.at[o % NY, c], sibling)

    def cross_recv(o, c):
        blk = xall.at[lane(o, other), chunk(c)]
        return rcopy(blk, blk, d2_send, d2_recv.at[o % NY, c], sibling)

    def expand(o, first=False):
        for c in range(2):
            cross_recv(o, c).wait_recv()
        yy = lax.rem(y + o + NY, NY)
        rows = jnp.concatenate(
            [flat(xall[2 * yy]), flat(xall[2 * yy + 1])], axis=1
        )
        ks = pl.ds(pl.multiple_of(yy * 2 * LANES, 2 * LANES), 2 * LANES)
        for acc, w in ((gate_acc, wg_v), (up_acc, wu_v)):
            prod = mm(rows, w[:, ks], (((1,), (1,)), ((), ())))
            if first:
                acc[...] = prod
            else:
                acc[...] += prod

    wait_bytes(outbox.at[pl.ds(0, (EP - 1) * UC)], disp_recv)
    for k in range(4):
        if streams[k][2] > 0:
            ring(k, 0).start()
    for c in range(2):
        cross(0, c).start()
    ready("x", "b", "c")
    last = pl.ds(L - LANES, LANES)
    halos = [
        rcopy(x_v.at[:, last], halo.at[pl.ds(0, VR)], halo_send.at[0], halo_recv.at[0], to_ep(1)),
        rcopy(b_v.at[:, last], halo.at[pl.ds(VR, NSTATE)], halo_send.at[1], halo_recv.at[1], to_ep(1)),
        rcopy(
            c_v.at[:, last], halo.at[pl.ds(VR + NSTATE, NSTATE)], halo_send.at[2], halo_recv.at[2], to_ep(1)
        ),
    ]
    for h in halos:
        h.start()
    ready("wg", "wu")

    started = (ep > 0).astype(F32)

    def conv(cur, rim, taps):
        joined = jnp.concatenate([rim.astype(F32) * started, cur.astype(F32)], axis=1)
        out = taps[:, 3:4] * joined[:, LANES:]
        for k in range(3):
            out = out + taps[:, k : k + 1] * pltpu.roll(joined, 3 - k, 1)[:, LANES:]
        return out * jax.nn.sigmoid(out)

    def state_part():
        for h in halos:
            h.wait_recv()

        ready("tapx", "tapb", "tapc", "hgain")
        taps_bc = jnp.transpose(jnp.concatenate([tapb_ref[:, gsel], tapc_ref[:, gsel]], axis=0))
        taps_x = jnp.transpose(
            jnp.concatenate([tapx_ref[...], hgain_ref[...], jnp.zeros((3, VR), F32)], axis=0)
        )
        b_conv = conv(b_v[...], halo[pl.ds(VR, NSTATE), :], taps_bc[:, :4]).astype(BF16)
        bc_v[...] = b_conv
        tail = jnp.exp(total - cum)
        for h in range(HH):
            rows_h = pl.ds(h * HD, HD)
            xc = conv(x_v[rows_h, :], halo[rows_h, :], taps_x[h * HD : (h + 1) * HD, :4])
            xs = xc * step[h : h + 1, :]
            xs_v[rows_h, :] = xs.astype(BF16)
            yloc[rows_h, :] = xs * tail[h : h + 1, :]
        state = mm(yloc[...].astype(BF16), b_conv, (((1,), (1,)), ((), ())))

        hi = total.astype(BF16).astype(F32)
        mid = (total - hi).astype(BF16).astype(F32)
        low = total - hi - mid
        r8 = lax.broadcasted_iota(jnp.int32, (8, LANES), 0)
        decays = []
        for u in range(EP):
            h = u * U // HD
            decays.append(
                jnp.where(
                    r8 == 0,
                    hi[h : h + 1],
                    jnp.where(r8 == 1, mid[h : h + 1], jnp.where(r8 == 2, low[h : h + 1], 0.0)),
                )
            )
        for u in range(EP):
            extra = [state[u * U : (u + 1) * U], decays[u]]
            if UR > U + 8:
                extra.append(jnp.zeros((UR - U - 8, LANES), F32))
            sout[u] = jnp.concatenate(extra, axis=0).astype(BF16)

        @pl.loop(1, EP)
        def _(d):
            tgt = lax.rem(ep + d, EP)
            rcopy(sout.at[tgt], sin.at[ep], st_send, st_recv, to_ep(d)).start()

        sin[ep] = sout[ep]
        return taps_x, taps_bc

    def local_part():
        c_conv = conv(c_v[...], halo[pl.ds(VR + NSTATE, NSTATE), :], taps[1][:, 4:]).astype(BF16)
        cc_v[...] = c_conv
        gram = mm(bc_v[...], c_conv, (((0,), (0,)), ((), ())))
        diag = lax.broadcasted_iota(jnp.int32, (LANES, LANES), 0) <= lax.broadcasted_iota(
            jnp.int32, (LANES, LANES), 1
        )
        for h in range(HH):
            for j in range(NB):
                at = cum_v[h : h + 1, j * LANES : (j + 1) * LANES]
                pieces = []
                for i in range(j + 1):
                    gap = at - colv[i * LANES : (i + 1) * LANES, h : h + 1]
                    if i == j:
                        gap = jnp.where(diag, gap, -jnp.inf)
                    g = gram[i * LANES : (i + 1) * LANES, j * LANES : (j + 1) * LANES]
                    pieces.append((g * jnp.exp(gap)).astype(BF16))
                weights = jnp.concatenate(pieces, axis=0) if j else pieces[0]
                rows_h = pl.ds(h * HD, HD)
                yloc[rows_h, j * LANES : (j + 1) * LANES] = mm(
                    xs_v[rows_h, : (j + 1) * LANES], weights
                )

    def prefix_part():
        wait_bytes(sout.at[pl.ds(0, EP - 1)], st_recv)
        held = jnp.zeros((U, LANES), F32)
        for e in range(EP):
            hout[e] = held
            blk = sin[e].astype(F32)
            keep = jnp.exp(blk[U : U + 1] + blk[U + 1 : U + 2] + blk[U + 2 : U + 3])
            held = keep * held + blk[:U]

        @pl.loop(1, EP)
        def _(d):
            tgt = lax.rem(ep + d, EP)
            rcopy(hout.at[tgt], hin.at[ep], hb_send, hb_recv, to_ep(d)).start()

        hin[ep] = hout[ep]

    def final_part():
        ready("z")
        wait_bytes(hout.at[pl.ds(0, EP - 1)], hb_recv)
        before = hin[...].reshape(VR, LANES).astype(BF16)
        for h in range(HH):
            rows_h = pl.ds(h * HD, HD)
            carried = mm(before[h * HD : (h + 1) * HD], cc_v[...]) * jnp.exp(cum_v[h : h + 1, :])
            z = z_v[rows_h, :].astype(F32)
            gated = (yloc[rows_h, :] + carried) * (z * jax.nn.sigmoid(z))
            scale = lax.rsqrt(jnp.mean(gated * gated, axis=0, keepdims=True) + HEAD_EPS)
            gain = taps[0][h * HD : (h + 1) * HD, 4:5]
            mixed_ref[rows_h, :] = (gated * scale * gain).astype(BF16)

    taps = []
    early = 1 if NY > 4 else 0
    fill_gather = {early: lambda: taps.extend(state_part()), early + 1: local_part}
    for i in range(NY // 2):
        if i in fill_gather:
            fill_gather[i]()
        expand(i, first=(i == 0))
        if i:
            expand(-i)
        for k in range(4):
            c, s, n = streams[k]
            if i < n:
                ring_recv(k, i).wait_recv()
                if i + 1 < n:
                    ring(k, i + 1).start()
                cross(-s * (i + 1), c).start()
    expand(NY // 2)

    gate = gate_acc[...]
    hid[...] = (gate * jax.nn.sigmoid(gate) * up_acc[...]).astype(BF16)

    ready("wd")

    def swap(o):
        return rcopy(part.at[o % NY, other], sib.at[o % NY], ps_send, ps_recv.at[o % NY], sibling)

    def project(o):
        yy = lax.rem(y + o + NY, NY)
        cols = pl.ds(pl.multiple_of(yy * 2 * LANES, 2 * LANES), 2 * LANES)
        prod = mm(hid[...], wd_v[:, cols]).astype(BF16)
        put(part.at[o % NY, 0], prod[:, :LANES])
        put(part.at[o % NY, 1], prod[:, LANES:])
        swap(o).start()

    swapped = set()

    def pair_sum(o, c):
        if o % NY not in swapped:
            swap(o).wait_recv()
            swapped.add(o % NY)
        mine = flat(part[o % NY, core, chunk(c)]).astype(F32)
        return mine + flat(sib[o % NY, chunk(c)]).astype(F32)

    slots, count = {}, 0
    for k in range(4):
        for i in range(streams[k][2]):
            slots[k, i] = count
            count += 1

    def push(k, i):
        j = slots[k, i]
        return rcopy(tosend.at[j], arrived.at[j], rs_send, rs_recv.at[j], to_y(streams[k][1]))

    def came(k, i):
        push(k, i).wait_recv()
        return flat(arrived[slots[k, i]]).astype(F32)

    reach = NY // 2
    project(reach)
    if reach > 1:
        project(reach - 1)
    fill_scatter = {min(1, reach - 1): prefix_part}
    for i in range(reach):
        for k in range(4):
            c, s, n = streams[k]
            if i == 0 and k == 2 and reach > 1:
                project(1 - reach)
            if i < n:
                value = pair_sum(s * (n - i), c)
                if i:
                    value = value + came(k, i - 1)
                put(tosend.at[slots[k, i]], value.astype(BF16))
                push(k, i).start()
        left = reach - 2 - i
        if left >= 0:
            project(left)
            if left:
                project(-left)
        if i in fill_scatter:
            fill_scatter[i]()
    if reach == 1:
        project(0)
    for c in range(2):
        value = pair_sum(0, c)
        for k in range(4):
            if streams[k][0] == c and streams[k][2] > 0:
                value = value + came(k, streams[k][2] - 1)
        put(rout.at[chunk(c)], value.astype(BF16))

    @pl.loop(1, EP)
    def _(d):
        tgt = lax.rem(ep + d, EP)
        rcopy(
            rout.at[pl.ds(tgt * UC, UC)], rin.at[pl.ds(ep * UC, UC)], rt_send, rt_recv, to_ep(d)
        ).start()

    rin[pl.ds(ep * UC, UC)] = rout[pl.ds(ep * UC, UC)]
    final_part()
    stores = [
        pltpu.make_async_copy(mixed_ref, mixed_hbm, store_sem.at[0]),
        pltpu.make_async_copy(moe_ref, moe_hbm, store_sem.at[1]),
    ]
    stores[0].start()
    wait_bytes(outbox.at[pl.ds(0, (EP - 1) * UC)], disp_send)
    for h in halos:
        h.wait_send()
    wait_bytes(sout.at[pl.ds(0, EP - 1)], st_send)
    wait_bytes(hout.at[pl.ds(0, EP - 1)], hb_send)
    wait_bytes(xall.at[pl.ds(0, NY - 1)], ag_send)
    wait_bytes(xall.at[pl.ds(0, NY)], d2_send)
    wait_bytes(sib, ps_send)
    wait_bytes(tosend, rs_send)

    wait_bytes(rout.at[pl.ds(0, (EP - 1) * UC)], rt_recv)
    back = flat(rin[...])
    moe_ref[...] = (mm(pick[0], back) + mm(pick[1], back)).astype(BF16)
    stores[1].start()
    for store in stores:
        store.wait()
    wait_bytes(rout.at[pl.ds(0, (EP - 1) * UC)], rt_send)


def place_body(mixed_ref, moe_ref, mixed_out, moe_out, sem):
    copies = [
        pltpu.make_async_copy(mixed_ref, mixed_out, sem.at[0]),
        pltpu.make_async_copy(moe_ref, moe_out, sem.at[1]),
    ]
    for copy in copies:
        copy.start()
    for copy in copies:
        copy.wait()


def on_device(EP, TP, *args):
    (x_in, z_in, dt_raw, decay_rate, b_in, c_in, conv_x, conv_b, conv_c, head_gain,
     moe_rows, moe_gain, routes, route_logit, w_gate, w_up, w_down) = args
    tokens, features = moe_rows.shape
    CAP = 2 * tokens * routes.shape[1] // EP
    VR, L = x_in.shape
    HH = dt_raw.shape[0]
    FD = w_gate.shape[2]
    flipped = functools.partial(jnp.swapaxes, axis1=-2, axis2=-1)
    NY = TP // 2
    ROWS = EP * CAP
    U = VR // EP
    UR = -(-(U + 8) // 16) * 16
    cfg = dict(EP=EP, TP=TP, CAP=CAP, L=L, HH=HH)
    hbm, vmem = (pl.BlockSpec(memory_space=m) for m in (pltpu.HBM, pltpu.VMEM))
    dma = pltpu.SemaphoreType.DMA
    units = (ROWS // QUAD, QUAD, LANES)
    half = (ROWS // QUAD // 2, QUAD, LANES)
    hops = 2 * (NY // 2) + 2 * (NY // 2 - 1)
    scratch = [
        pltpu.VMEM((HH, L), F32), pltpu.VMEM((1, HH), F32),
        pltpu.VMEM((4, VR), F32), pltpu.VMEM((4, conv_b.shape[0]), F32), pltpu.VMEM((4, conv_b.shape[0]), F32),
        pltpu.VMEM((1, VR), F32), pltpu.VMEM((TP, features // TP), F32),
        pltpu.VMEM((2, tokens), jnp.int32), pltpu.VMEM((2, tokens), F32),
        pltpu.VMEM((VR, L), BF16), pltpu.VMEM((tokens, features // TP), BF16),
        pltpu.VMEM((VR, L), BF16), pltpu.VMEM((VR, L), BF16),
        pltpu.VMEM((NSTATE, L), BF16), pltpu.VMEM((NSTATE, L), BF16),
        pltpu.VMEM((tokens, features), BF16),
        pltpu.VMEM((FD, features), BF16), pltpu.VMEM((FD, features), BF16), pltpu.VMEM((FD, features), BF16),
        pltpu.VMEM((VR + 2 * NSTATE, LANES), BF16),
        pltpu.VMEM((2, tokens, ROWS), BF16),
        pltpu.VMEM(units, BF16), pltpu.VMEM((TP,) + units, BF16),
        pltpu.VMEM((ROWS, FD), F32), pltpu.VMEM((ROWS, FD), F32), pltpu.VMEM((ROWS, FD), BF16),
        pltpu.VMEM((NY, 2) + units, BF16), pltpu.VMEM((NY,) + units, BF16),
        pltpu.VMEM((hops,) + half, BF16), pltpu.VMEM((hops,) + half, BF16),
        pltpu.VMEM(units, BF16), pltpu.VMEM(units, BF16),
        pltpu.VMEM((VR, L), BF16), pltpu.VMEM((NSTATE, L), BF16), pltpu.VMEM((NSTATE, L), BF16),
        pltpu.VMEM((8, L), F32), pltpu.VMEM((L, 8), F32), pltpu.VMEM((VR, L), F32),
        pltpu.VMEM((EP, UR, LANES), BF16), pltpu.VMEM((EP, UR, LANES), BF16),
        pltpu.VMEM((EP, U, LANES), F32), pltpu.VMEM((EP, U, LANES), F32),
        dma((17,)), dma((2,)), dma((3,)), dma((3,)), dma, dma, dma, dma, dma, dma,
        dma, dma((4, NY // 2)), dma, dma((NY, 2)), dma, dma((NY,)), dma, dma((hops,)), dma, dma,
    ]
    outs = pl.pallas_call(
        functools.partial(kernel_body, cfg),
        name="mixer_and_experts",
        out_shape=(
            jax.ShapeDtypeStruct((VR, L), BF16),
            jax.ShapeDtypeStruct((tokens, features // TP), BF16),
        ),
        in_specs=[hbm] * 17,
        out_specs=(hbm, hbm),
        scratch_shapes=scratch,
        compiler_params=pltpu.CompilerParams(
            collective_id=0, has_side_effects=True, vmem_limit_bytes=60 * 1024 * 1024
        ),
    )(
        x_in, z_in, dt_raw, decay_rate.reshape(1, HH), b_in, c_in, flipped(conv_x), flipped(conv_b), flipped(conv_c),
        head_gain.reshape(1, VR), moe_rows, moe_gain.reshape(TP, features // TP),
        flipped(routes), flipped(route_logit), flipped(w_gate), flipped(w_up), w_down,
    )
    mixed, moe = pl.pallas_call(
        place_body,
        name="place",
        out_shape=tuple(jax.ShapeDtypeStruct(o.shape, o.dtype) for o in outs),
        in_specs=[vmem, vmem],
        out_specs=(hbm, hbm),
        scratch_shapes=[dma((2,))],
    )(*outs)
    return mixed, flipped(moe)


def solution(mesh):
    EP, TP = mesh.shape["ep"], mesh.shape["tp"]
    in_specs = (
        P("tp", "ep"), P("tp", "ep"), P("tp", "ep"), P("tp"), P(None, "ep"), P(None, "ep"),
        P("tp", None), P(), P(), P("tp"), P("ep", None), P(), P("ep", None), P("ep", None),
        P("ep", None, "tp"), P("ep", None, "tp"), P("ep", "tp", None),
    )
    return jax.shard_map(
        functools.partial(on_device, EP, TP),
        mesh=mesh,
        in_specs=in_specs,
        out_specs=(P("tp", "ep"), P("tp", "ep")),
        check_vma=False,
    )
```

```python
import functools

import jax
import jax.numpy as jnp
from jax import lax
from jax.experimental import pallas as pl
from jax.experimental.pallas import tpu as pltpu
from jax.sharding import PartitionSpec as P

F32 = jnp.float32
BF16 = jnp.bfloat16
MESH = pl.DeviceIdType.MESH
HIGHEST = lax.Precision.HIGHEST
GROUPS = 2
NSTATE = 128
LANES = 128
QUAD = 4
ROW_EPS = 0.1
HEAD_EPS = 1.0


def mm(a, b, dims=(((1,), (0,)), ((), ()))):
    return lax.dot_general(a, b, dims, preferred_element_type=F32)


def kernel_body(
    cfg,
    x_hbm, z_hbm, dt_hbm, rate_hbm, b_hbm, c_hbm, tapx_hbm, tapb_hbm, tapc_hbm, hgain_hbm,
    rows_hbm, mgain_hbm, routes_hbm, logit_hbm, wg_hbm, wu_hbm, wd_hbm,
    mixed_ref, moe_ref,
    dt_ref, rate_ref, tapx_ref, tapb_ref, tapc_ref, hgain_ref, mgain_ref, routes_ref, logit_ref,
    x_v, z_v, b_v, c_v, rows_v, wg_v, wu_v, wd_v, halo, pick, outbox, inbox, xall,
    gate_acc, up_acc, hid, part, sib, tosend, arrived, rout, rin,
    xs_v, bc_v, cc_v, gram_v, cum_v, colv, yloc, sout, sin, hout, hin,
    load_sem, halo_send, halo_recv, disp_send, disp_recv, st_send, st_recv, hb_send, hb_recv,
    ag_send, ag_recv, d2_send, d2_recv, ps_send, ps_recv, rs_send, rs_recv, rt_send, rt_recv,
):
    EP, TP, CAP, L, HH = cfg["EP"], cfg["TP"], cfg["CAP"], cfg["L"], cfg["HH"]
    NY = TP // 2
    UC = CAP // QUAD
    ROWS = EP * CAP
    half_rows, quarter = ROWS // 2, ROWS // 4
    tokens = rows_v.shape[0]
    VR = x_v.shape[0]
    HD = VR // HH
    NB = L // LANES
    U = VR // EP
    UR = sout.shape[1]
    ep, tp = lax.axis_index("ep"), lax.axis_index("tp")
    y, core = lax.div(tp, 2), lax.rem(tp, 2)
    other = 1 - core
    group = lax.div(tp, TP // GROUPS)

    NX = min(4, EP)
    NZ = EP // NX
    z_at, x_at = lax.div(ep, NX), lax.rem(ep, NX)

    def hops(offset):
        dz, dx = offset
        return min(dz, NZ - dz) + min(dx, NX - dx)

    offsets = sorted(((dz, dx) for dz in range(NZ) for dx in range(NX) if dz or dx), key=lambda o: -hops(o))
    partners = [lax.rem(z_at + dz, NZ) * NX + lax.rem(x_at + dx, NX) for dz, dx in offsets]

    def at_ep(index):
        return {"ep": index, "tp": tp}

    def to_y(s):
        return {"ep": ep, "tp": lax.rem(y + s + NY, NY) * 2 + core}

    sibling = {"ep": ep, "tp": y * 2 + other}

    def rcopy(src, dst, ssem, rsem, dev):
        return pltpu.make_async_remote_copy(
            src_ref=src, dst_ref=dst, send_sem=ssem, recv_sem=rsem, device_id=dev, device_id_type=MESH
        )

    def flat(block):
        return block.reshape(block.shape[0] * QUAD, LANES)

    def put(ref, value):
        ref[...] = value.reshape(value.shape[0] // QUAD, QUAD, LANES)

    def wait_bytes(ref, sem):
        pltpu.make_async_copy(ref, ref, sem).wait()

    barrier = pltpu.get_barrier_semaphore()

    for tgt in partners:
        pl.semaphore_signal(barrier, inc=1, device_id=at_ep(tgt), device_id_type=MESH)

    for dev in (to_y(1), to_y(-1), sibling):
        pl.semaphore_signal(barrier, inc=1, device_id=dev, device_id_type=MESH)

    gsel = pl.ds(pl.multiple_of(group * NSTATE, NSTATE), NSTATE)
    loads = {}
    for i, (name, src, dst) in enumerate(
        (
            ("routes", routes_hbm, routes_ref), ("rows", rows_hbm, rows_v), ("mgain", mgain_hbm, mgain_ref),
            ("logit", logit_hbm, logit_ref), ("dt", dt_hbm, dt_ref), ("rate", rate_hbm, rate_ref),
            ("x", x_hbm, x_v), ("b", b_hbm.at[gsel, :], b_v), ("c", c_hbm.at[gsel, :], c_v),
            ("tapx", tapx_hbm, tapx_ref), ("tapb", tapb_hbm, tapb_ref), ("tapc", tapc_hbm, tapc_ref),
            ("hgain", hgain_hbm, hgain_ref),
            ("wg", wg_hbm.at[0], wg_v), ("wu", wu_hbm.at[0], wu_v), ("wd", wd_hbm.at[0], wd_v),
            ("z", z_hbm, z_v),
        )
    ):
        loads[name] = pltpu.make_async_copy(src, dst, load_sem.at[i])
        loads[name].start()

    def ready(*names):
        for name in names:
            loads[name].wait()

    ready("routes")
    routes = routes_ref[...]
    row_e = lax.broadcasted_iota(jnp.int32, (EP, tokens), 0)
    hits = [(routes[k : k + 1, :] == row_e).astype(F32) for k in range(2)]
    before = (
        lax.broadcasted_iota(jnp.int32, (tokens, tokens), 0)
        < lax.broadcasted_iota(jnp.int32, (tokens, tokens), 1)
    ).astype(BF16)
    ahead = mm((hits[0] + hits[1]).astype(BF16), before)
    row_s = lax.broadcasted_iota(jnp.int32, (ROWS, tokens), 0)
    hots = []
    for k in range(2):
        rank = jnp.sum(ahead * hits[k], axis=0, keepdims=True).astype(jnp.int32)
        hots.append(row_s == routes[k : k + 1, :] * CAP + rank)
    onehot = (hots[0] | hots[1]).astype(F32).astype(BF16)

    ready("rows", "mgain")
    rows_f = rows_v[...].astype(F32)
    row_scale = lax.rsqrt(jnp.mean(rows_f * rows_f, axis=1, keepdims=True) + ROW_EPS)
    own_cols = rows_v[:, pl.ds(pl.multiple_of(tp * LANES, LANES), LANES)].astype(F32)
    normed = (own_cols * row_scale * mgain_ref[pl.ds(tp, 1), :]).astype(BF16)
    packed = mm(onehot, normed).astype(BF16)
    put(outbox, packed)

    pl.semaphore_wait(barrier, EP - 1 + 3)

    for tgt in partners:
        rcopy(
            outbox.at[pl.ds(tgt * UC, UC)], inbox.at[pl.ds(ep * UC, UC)], disp_send, disp_recv, at_ep(tgt)
        ).start()

    inbox[pl.ds(ep * UC, UC)] = outbox[pl.ds(ep * UC, UC)]

    ready("logit", "dt", "rate")
    logit = logit_ref[...]
    share = jax.nn.sigmoid(logit[0:1, :] - logit[1:2, :])
    weighted = jnp.where(hots[0], share, jnp.where(hots[1], jax.nn.sigmoid(logit[1:2, :] - logit[0:1, :]), 0.0))
    weighted = jnp.transpose(weighted)
    coarse = weighted.astype(BF16)
    pick[0] = coarse
    pick[1] = (weighted - coarse.astype(F32)).astype(BF16)

    dt = dt_ref[...]
    step = jnp.maximum(dt, 0.0) + jnp.log1p(jnp.exp(-jnp.abs(dt)))
    eye = lax.broadcasted_iota(jnp.int32, (HH, HH), 0) == lax.broadcasted_iota(jnp.int32, (HH, HH), 1)
    rate = jnp.sum(jnp.where(eye, rate_ref[...], 0.0), axis=1, keepdims=True)
    logd = -step * rate
    upper = (
        lax.broadcasted_iota(jnp.int32, (LANES, LANES), 0)
        <= lax.broadcasted_iota(jnp.int32, (LANES, LANES), 1)
    ).astype(F32)
    pieces, carry = [], jnp.zeros((HH, 1), F32)
    for k in range(NB):
        piece = (
            jnp.dot(
                logd[:, k * LANES : (k + 1) * LANES], upper, precision=HIGHEST, preferred_element_type=F32
            )
            + carry
        )
        carry = piece[:, LANES - 1 : LANES]
        pieces.append(piece)
    cum = jnp.concatenate(pieces, axis=1)
    total = carry
    cum_v[pl.ds(0, HH), :] = cum
    tall = jnp.concatenate([cum, jnp.zeros((8 - HH, L), F32)], axis=0)
    colv[...] = jnp.transpose(tall)

    reach = NY // 2
    streams = []
    for q in range(4):
        streams.append((q, 1, reach - q % 2))
        streams.append((q, -1, reach - 1 + q % 2))

    def lane(o, c):
        return lax.rem(y + o + NY, NY) * 2 + c

    def part_of(q):
        return pl.ds(q * quarter, quarter)

    def half_of(h):
        return pl.ds(h * half_rows, half_rows)

    phases = ((0, 3), (4, 7), (1, 2), (5, 6))
    slots, count = {}, 0
    for k in range(8):
        for i in range(streams[k][2]):
            slots[k, i] = count
            count += 1

    def live(p, i):
        return [k for k in phases[p] if i < streams[k][2]]

    def ring(k, i):
        q, s, _ = streams[k]
        blk = xall.at[lane(-s * i, core), part_of(q)]
        return rcopy(blk, blk, ag_send, ag_recv.at[slots[k, i]], to_y(s))

    def ring_recv(k, i):
        q, s, _ = streams[k]
        blk = xall.at[lane(-s * (i + 1), core), part_of(q)]
        return rcopy(blk, blk, ag_send, ag_recv.at[slots[k, i]], to_y(s))

    def cross(o, q):
        blk = xall.at[lane(o, core), part_of(q)]
        return rcopy(blk, blk, d2_send, d2_recv.at[o % NY, q // 2], sibling)

    def cross_half(o, h, c):
        blk = xall.at[lane(o, c), half_of(h)]
        return rcopy(blk, blk, d2_send, d2_recv.at[o % NY, h], sibling)

    def drain(i, p):
        for k in live(p, i):
            q, s, n = streams[k]
            ring_recv(k, i).wait_recv()
            if i + 1 < n:
                ring(k, i + 1).start()
            cross(-s * (i + 1), q).start()

    def expand(o, h, first=False):
        cross_half(o, h, other).wait_recv()
        yy = lax.rem(y + o + NY, NY)
        rows = jnp.concatenate([xall[2 * yy, half_of(h), :], xall[2 * yy + 1, half_of(h), :]], axis=1)
        ks = pl.ds(pl.multiple_of(yy * 2 * LANES, 2 * LANES), 2 * LANES)
        for acc, w in ((gate_acc, wg_v), (up_acc, wu_v)):
            prod = mm(rows, w[:, ks], (((1,), (1,)), ((), ())))
            if first:
                acc[half_of(h), :] = prod
            else:
                acc[half_of(h), :] += prod

    wait_bytes(outbox.at[pl.ds(0, (EP - 1) * UC)], disp_recv)
    xall[tp] = flat(inbox[...])
    for p in range(4):
        for k in live(p, 0):
            ring(k, 0).start()
    for h in range(2):
        cross_half(0, h, core).start()
    ready("x", "b", "c")
    last = pl.ds(L - LANES, LANES)
    halos = [
        rcopy(x_v.at[:, last], halo.at[pl.ds(0, VR)], halo_send.at[0], halo_recv.at[0], at_ep(lax.rem(ep + 1, EP))),
        rcopy(b_v.at[:, last], halo.at[pl.ds(VR, NSTATE)], halo_send.at[1], halo_recv.at[1], at_ep(lax.rem(ep + 1, EP))),
        rcopy(
            c_v.at[:, last], halo.at[pl.ds(VR + NSTATE, NSTATE)], halo_send.at[2], halo_recv.at[2], at_ep(lax.rem(ep + 1, EP))
        ),
    ]
    for h in halos:
        h.start()
    ready("wg", "wu")

    started = (ep > 0).astype(F32)

    def conv(cur, rim, taps):
        joined = jnp.concatenate([rim.astype(F32) * started, cur.astype(F32)], axis=1)
        out = taps[:, 3:4] * joined[:, LANES:]
        for k in range(3):
            out = out + taps[:, k : k + 1] * pltpu.roll(joined, 3 - k, 1)[:, LANES:]
        return out * jax.nn.sigmoid(out)

    kept = {}

    def taps_part():
        for h in halos:
            h.wait_recv()
        ready("tapx", "tapb", "tapc", "hgain")
        kept["bc"] = jnp.transpose(jnp.concatenate([tapb_ref[:, gsel], tapc_ref[:, gsel]], axis=0))
        kept["x"] = jnp.transpose(
            jnp.concatenate([tapx_ref[...], hgain_ref[...], jnp.zeros((3, VR), F32)], axis=0)
        )
        bc_v[...] = conv(b_v[...], halo[pl.ds(VR, NSTATE), :], kept["bc"][:, :4]).astype(BF16)

    def value_part(heads):
        tail = jnp.exp(total - cum)
        for h in heads:
            rows_h = pl.ds(h * HD, HD)
            xc = conv(x_v[rows_h, :], halo[rows_h, :], kept["x"][h * HD : (h + 1) * HD, :4])
            xs = xc * step[h : h + 1, :]
            xs_v[rows_h, :] = xs.astype(BF16)
            yloc[rows_h, :] = xs * tail[h : h + 1, :]

    def send_part():
        state = mm(yloc[...].astype(BF16), bc_v[...], (((1,), (1,)), ((), ())))
        hi = total.astype(BF16).astype(F32)
        mid = (total - hi).astype(BF16).astype(F32)
        low = total - hi - mid
        r8 = lax.broadcasted_iota(jnp.int32, (8, LANES), 0)
        for u in range(EP):
            h = u * U // HD
            decay = jnp.where(
                r8 == 0,
                hi[h : h + 1],
                jnp.where(r8 == 1, mid[h : h + 1], jnp.where(r8 == 2, low[h : h + 1], 0.0)),
            )
            extra = [state[u * U : (u + 1) * U], decay]
            if UR > U + 8:
                extra.append(jnp.zeros((UR - U - 8, LANES), F32))
            sout[u] = jnp.concatenate(extra, axis=0).astype(BF16)

        @pl.loop(1, EP)
        def _(d):
            tgt = lax.rem(ep + d, EP)
            rcopy(sout.at[tgt], sin.at[ep], st_send, st_recv, at_ep(tgt)).start()

        sin[ep] = sout[ep]

    def gram_part():
        c_conv = conv(c_v[...], halo[pl.ds(VR + NSTATE, NSTATE), :], kept["bc"][:, 4:]).astype(BF16)
        cc_v[...] = c_conv
        gram_v[...] = mm(bc_v[...], c_conv, (((0,), (0,)), ((), ())))

    def local_part(heads):
        diag = lax.broadcasted_iota(jnp.int32, (LANES, LANES), 0) <= lax.broadcasted_iota(
            jnp.int32, (LANES, LANES), 1
        )
        for h in heads:
            for j in range(NB):
                at = cum_v[h : h + 1, j * LANES : (j + 1) * LANES]
                pieces = []
                for i in range(j + 1):
                    gap = at - colv[i * LANES : (i + 1) * LANES, h : h + 1]
                    if i == j:
                        gap = jnp.where(diag, gap, -jnp.inf)
                    g = gram_v[i * LANES : (i + 1) * LANES, j * LANES : (j + 1) * LANES]
                    pieces.append((g * jnp.exp(gap)).astype(BF16))
                weights = jnp.concatenate(pieces, axis=0) if j else pieces[0]
                rows_h = pl.ds(h * HD, HD)
                yloc[rows_h, j * LANES : (j + 1) * LANES] = mm(
                    xs_v[rows_h, : (j + 1) * LANES], weights
                )

    def prefix_part():
        wait_bytes(sout.at[pl.ds(0, EP - 1)], st_recv)
        held = jnp.zeros((U, LANES), F32)
        for e in range(EP):
            hout[e] = held
            blk = sin[e].astype(F32)
            keep = jnp.exp(blk[U : U + 1] + blk[U + 1 : U + 2] + blk[U + 2 : U + 3])
            held = keep * held + blk[:U]

        @pl.loop(1, EP)
        def _(d):
            tgt = lax.rem(ep + d, EP)
            rcopy(hout.at[tgt], hin.at[ep], hb_send, hb_recv, at_ep(tgt)).start()

        hin[ep] = hout[ep]

    def final_part():
        ready("z")
        wait_bytes(hout.at[pl.ds(0, EP - 1)], hb_recv)
        before = hin[...].reshape(VR, LANES).astype(BF16)
        for h in range(HH):
            rows_h = pl.ds(h * HD, HD)
            carried = mm(before[h * HD : (h + 1) * HD], cc_v[...]) * jnp.exp(cum_v[h : h + 1, :])
            z = z_v[rows_h, :].astype(F32)
            gated = (yloc[rows_h, :] + carried) * (z * jax.nn.sigmoid(z))
            scale = lax.rsqrt(jnp.mean(gated * gated, axis=0, keepdims=True) + HEAD_EPS)
            gain = kept["x"][h * HD : (h + 1) * HD, 4:5]
            mixed_ref[rows_h, :] = (gated * scale * gain).astype(BF16)

    pieces = [
        taps_part,
        lambda: value_part(range(HH // 2)),
        lambda: value_part(range(HH // 2, HH)),
        send_part,
        gram_part,
        lambda: local_part([0]),
        lambda: local_part([1]),
        lambda: local_part(range(2, HH)),
    ]

    for h in range(2):
        expand(0, h, first=True)
    far = reach - 1
    for i in range(far):
        for p in range(4):
            drain(i, p)
            if i:
                expand((i, -i, i, -i)[p], p // 2)
            if (i or p > 1) and pieces:
                pieces.pop(0)()
    if far:
        expand(far, 0)
    for piece in pieces:
        piece()
    drain(far, 0)
    if far:
        expand(-far, 0)
    drain(far, 1)
    if far:
        expand(far, 1)
        expand(-far, 1)

    ready("wd")

    def activate(h):
        gate = gate_acc[half_of(h), :]
        hid[half_of(h), :] = (gate * jax.nn.sigmoid(gate) * up_acc[half_of(h), :]).astype(BF16)

    def swap(o, h):
        return rcopy(
            part.at[o % NY, other, half_of(h)], sib.at[o % NY, half_of(h)], ps_send, ps_recv.at[o % NY, h], sibling
        )

    def project(o, h):
        yy = lax.rem(y + o + NY, NY)
        cols = pl.ds(pl.multiple_of(yy * 2 * LANES, 2 * LANES), 2 * LANES)
        prod = mm(hid[half_of(h), :], wd_v[:, cols]).astype(BF16)
        part[o % NY, 0, half_of(h), :] = prod[:, :LANES]
        part[o % NY, 1, half_of(h), :] = prod[:, LANES:]
        swap(o, h).start()

    swapped = set()

    def pair_sum(o, q):
        at = (o % NY, q // 2)
        if at not in swapped:
            swap(*at).wait_recv()
            swapped.add(at)
        mine = part[o % NY, core, part_of(q), :].astype(F32)
        return mine + sib[o % NY, part_of(q), :].astype(F32)

    def push(k, i):
        j = slots[k, i]
        return rcopy(tosend.at[j], arrived.at[j], rs_send, rs_recv.at[j], to_y(streams[k][1]))

    def came(k, i):
        push(k, i).wait_recv()
        return arrived[slots[k, i]].astype(F32)

    def feed(k, i):
        q, s, n = streams[k]
        value = pair_sum(s * (n - i), q)
        if i:
            value = value + came(k, i - 1)
        tosend[slots[k, i]] = value.astype(BF16)
        push(k, i).start()

    def feed_all(p, i):
        for k in live(p, i):
            feed(k, i)

    def project_for(i, side, h):
        m = reach - 1 - i
        if m > 0:
            project(side * m, h)
        elif m == 0 and side < 0:
            project(0, h)

    for h in range(2):
        expand(reach, h)
        activate(h)
        project(reach, h)
    feed_all(0, 0)
    project_for(0, -1, 0)
    feed_all(1, 0)
    project_for(0, 1, 0)
    project_for(0, -1, 1)
    project_for(0, 1, 1)
    feed_all(2, 0)
    project_for(1, -1, 0)
    feed_all(3, 0)
    project_for(1, 1, 0)
    for i in range(1, reach):
        for p in range(4):
            feed_all(p, i)
            if p < 2:
                project_for(i, (-1, 1)[p], 1)
            else:
                project_for(i + 1, (-1, 1)[p - 2], 0)
            if (i, p) == (min(2, far), 1):
                prefix_part()
    if reach == 1:
        project(0, 1)
    units = quarter // QUAD
    for q in range(4):
        value = pair_sum(0, q)
        for k in (2 * q, 2 * q + 1):
            if streams[k][2] > 0:
                value = value + came(k, streams[k][2] - 1)
        put(rout.at[pl.ds(q * units, units)], value.astype(BF16))

    for tgt in partners:
        rcopy(
            rout.at[pl.ds(tgt * UC, UC)], rin.at[pl.ds(ep * UC, UC)], rt_send, rt_recv, at_ep(tgt)
        ).start()

    rin[pl.ds(ep * UC, UC)] = rout[pl.ds(ep * UC, UC)]
    final_part()
    wait_bytes(outbox.at[pl.ds(0, (EP - 1) * UC)], disp_send)
    for h in halos:
        h.wait_send()
    wait_bytes(sout.at[pl.ds(0, EP - 1)], st_send)
    wait_bytes(hout.at[pl.ds(0, EP - 1)], hb_send)
    wait_bytes(xall.at[pl.ds(0, NY - 1)], ag_send)
    wait_bytes(xall.at[pl.ds(0, NY)], d2_send)
    wait_bytes(sib, ps_send)
    wait_bytes(tosend, rs_send)

    wait_bytes(rout.at[pl.ds(0, (EP - 1) * UC)], rt_recv)
    back = flat(rin[...])
    moe_ref[...] = (mm(pick[0], back) + mm(pick[1], back)).astype(BF16)
    wait_bytes(rout.at[pl.ds(0, (EP - 1) * UC)], rt_send)


def on_device(EP, TP, *args):
    (x_in, z_in, dt_raw, decay_rate, b_in, c_in, conv_x, conv_b, conv_c, head_gain,
     moe_rows, moe_gain, routes, route_logit, w_gate, w_up, w_down) = args
    tokens, features = moe_rows.shape
    CAP = 2 * tokens * routes.shape[1] // EP
    VR, L = x_in.shape
    HH = dt_raw.shape[0]
    FD = w_gate.shape[2]
    flipped = functools.partial(jnp.swapaxes, axis1=-2, axis2=-1)
    NY = TP // 2
    ROWS = EP * CAP
    U = VR // EP
    UR = -(-(U + 8) // 16) * 16
    cfg = dict(EP=EP, TP=TP, CAP=CAP, L=L, HH=HH)
    hbm, vmem = (pl.BlockSpec(memory_space=m) for m in (pltpu.HBM, pltpu.VMEM))
    dma = pltpu.SemaphoreType.DMA
    units = (ROWS // QUAD, QUAD, LANES)
    block = (ROWS, LANES)
    piece = (ROWS // 4, LANES)
    hops = 4 * (2 * (NY // 2) - 1)
    scratch = [
        pltpu.VMEM((HH, L), F32), pltpu.VMEM((1, HH), F32),
        pltpu.VMEM((4, VR), F32), pltpu.VMEM((4, conv_b.shape[0]), F32), pltpu.VMEM((4, conv_b.shape[0]), F32),
        pltpu.VMEM((1, VR), F32), pltpu.VMEM((TP, features // TP), F32),
        pltpu.VMEM((2, tokens), jnp.int32), pltpu.VMEM((2, tokens), F32),
        pltpu.VMEM((VR, L), BF16), pltpu.VMEM((VR, L), BF16),
        pltpu.VMEM((NSTATE, L), BF16), pltpu.VMEM((NSTATE, L), BF16),
        pltpu.VMEM((tokens, features), BF16),
        pltpu.VMEM((FD, features), BF16), pltpu.VMEM((FD, features), BF16), pltpu.VMEM((FD, features), BF16),
        pltpu.VMEM((VR + 2 * NSTATE, LANES), BF16),
        pltpu.VMEM((2, tokens, ROWS), BF16),
        pltpu.VMEM(units, BF16), pltpu.VMEM(units, BF16), pltpu.VMEM((TP,) + block, BF16),
        pltpu.VMEM((ROWS, FD), F32), pltpu.VMEM((ROWS, FD), F32), pltpu.VMEM((ROWS, FD), BF16),
        pltpu.VMEM((NY, 2) + block, BF16), pltpu.VMEM((NY,) + block, BF16),
        pltpu.VMEM((hops,) + piece, BF16), pltpu.VMEM((hops,) + piece, BF16),
        pltpu.VMEM(units, BF16), pltpu.VMEM(units, BF16),
        pltpu.VMEM((VR, L), BF16), pltpu.VMEM((NSTATE, L), BF16), pltpu.VMEM((NSTATE, L), BF16),
        pltpu.VMEM((L, L), F32), pltpu.VMEM((8, L), F32), pltpu.VMEM((L, 8), F32), pltpu.VMEM((VR, L), F32),
        pltpu.VMEM((EP, UR, LANES), BF16), pltpu.VMEM((EP, UR, LANES), BF16),
        pltpu.VMEM((EP, U, LANES), F32), pltpu.VMEM((EP, U, LANES), F32),
        dma((17,)), dma((3,)), dma((3,)), dma, dma, dma, dma, dma, dma,
        dma, dma((hops,)), dma, dma((NY, 2)), dma, dma((NY, 2)), dma, dma((hops,)), dma, dma,
    ]
    mixed, moe = pl.pallas_call(
        functools.partial(kernel_body, cfg),
        name="mixer_and_experts",
        out_shape=(
            pltpu.VMEM((VR, L), BF16),
            pltpu.VMEM((tokens, features // TP), BF16),
        ),
        in_specs=[hbm] * 17,
        out_specs=(vmem, vmem),
        scratch_shapes=scratch,
        compiler_params=pltpu.CompilerParams(
            collective_id=0, has_side_effects=True, vmem_limit_bytes=60 * 1024 * 1024
        ),
    )(
        x_in, z_in, dt_raw, decay_rate.reshape(1, HH), b_in, c_in, flipped(conv_x), flipped(conv_b), flipped(conv_c),
        head_gain.reshape(1, VR), moe_rows, moe_gain.reshape(TP, features // TP),
        flipped(routes), flipped(route_logit), flipped(w_gate), flipped(w_up), w_down,
    )
    return mixed, flipped(moe)


def solution(mesh):
    EP, TP = mesh.shape["ep"], mesh.shape["tp"]
    in_specs = (
        P("tp", "ep"), P("tp", "ep"), P("tp", "ep"), P("tp"), P(None, "ep"), P(None, "ep"),
        P("tp", None), P(), P(), P("tp"), P("ep", None), P(), P("ep", None), P("ep", None),
        P("ep", None, "tp"), P("ep", None, "tp"), P("ep", "tp", None),
    )
    return jax.shard_map(
        functools.partial(on_device, EP, TP),
        mesh=mesh,
        in_specs=in_specs,
        out_specs=(P("tp", "ep"), P("tp", "ep")),
        check_vma=False,
    )
```

```python
import functools

import jax
import jax.numpy as jnp
from jax import lax
from jax.experimental import pallas as pl
from jax.experimental.pallas import tpu as pltpu
from jax.sharding import PartitionSpec as P

F32 = jnp.float32
BF16 = jnp.bfloat16
MESH = pl.DeviceIdType.MESH
HIGHEST = lax.Precision.HIGHEST
GROUPS = 2
NSTATE = 128
LANES = 128
QUAD = 4
ROW_EPS = 0.1
HEAD_EPS = 1.0


def mm(a, b, dims=(((1,), (0,)), ((), ()))):
    return lax.dot_general(a, b, dims, preferred_element_type=F32)


def kernel_body(
    cfg,
    x_hbm, z_hbm, dt_hbm, rate_hbm, b_hbm, c_hbm, tapx_hbm, tapb_hbm, tapc_hbm, hgain_hbm,
    rows_hbm, mgain_hbm, routes_hbm, logit_hbm, wg_hbm, wu_hbm, wd_hbm,
    mixed_ref, moe_ref,
    dt_ref, rate_ref, tapx_ref, tapb_ref, tapc_ref, hgain_ref, mgain_ref, routes_ref, logit_ref,
    x_v, z_v, b_v, c_v, rows_v, wg_v, wu_v, wd_v, halo, rim_out, rim_in, pick, outbox, inbox, xall,
    gate_acc, up_acc, hid, part, sib, tosend, arrived, rout, rin,
    xs_v, bc_v, cc_v, gram_v, cum_v, colv, yloc, sout, sin, hout, hin,
    load_sem, halo_send, halo_recv, disp_send, disp_recv, st_send, st_recv, hb_send, hb_recv,
    ag_send, ag_recv, d2_send, d2_recv, ps_send, ps_recv, rs_send, rs_recv, rt_send, rt_recv,
):
    EP, TP, CAP, L, HH = cfg["EP"], cfg["TP"], cfg["CAP"], cfg["L"], cfg["HH"]
    NY = TP // 2
    UC = CAP // QUAD
    ROWS = EP * CAP
    half_rows, quarter = ROWS // 2, ROWS // 4
    tokens = rows_v.shape[0]
    VR = x_v.shape[0]
    HD = VR // HH
    NB = L // LANES
    U = VR // EP
    UR = sout.shape[1]
    ep, tp = lax.axis_index("ep"), lax.axis_index("tp")
    y, core = lax.div(tp, 2), lax.rem(tp, 2)
    other = 1 - core
    group = lax.div(tp, TP // GROUPS)

    NX = min(4, EP)
    NZ = EP // NX
    z_at, x_at = lax.div(ep, NX), lax.rem(ep, NX)

    def hops(offset):
        dz, dx = offset
        return min(dz, NZ - dz) + min(dx, NX - dx)

    ranked = sorted(((dz, dx) for dz in range(NZ) for dx in range(NX)), key=hops)
    seat = {offset: i for i, offset in enumerate(ranked)}
    offsets = ranked[:0:-1]
    partners = [lax.rem(z_at + dz, NZ) * NX + lax.rem(x_at + dx, NX) for dz, dx in offsets]

    def at_ep(index):
        return {"ep": index, "tp": tp}

    def to_y(s):
        return {"ep": ep, "tp": lax.rem(y + s + NY, NY) * 2 + core}

    sibling = {"ep": ep, "tp": y * 2 + other}

    def rcopy(src, dst, ssem, rsem, dev):
        return pltpu.make_async_remote_copy(
            src_ref=src, dst_ref=dst, send_sem=ssem, recv_sem=rsem, device_id=dev, device_id_type=MESH
        )

    def flat(block):
        return block.reshape(block.shape[0] * QUAD, LANES)

    def put(ref, value):
        ref[...] = value.reshape(value.shape[0] // QUAD, QUAD, LANES)

    def wait_bytes(ref, sem):
        pltpu.make_async_copy(ref, ref, sem).wait()

    barrier = pltpu.get_barrier_semaphore()

    for tgt in partners:
        pl.semaphore_signal(barrier, inc=1, device_id=at_ep(tgt), device_id_type=MESH)

    for dev in (to_y(1), to_y(-1), sibling):
        pl.semaphore_signal(barrier, inc=1, device_id=dev, device_id_type=MESH)

    gsel = pl.ds(pl.multiple_of(group * NSTATE, NSTATE), NSTATE)
    loads = {}
    for i, (name, src, dst) in enumerate(
        (
            ("routes", routes_hbm, routes_ref), ("rows", rows_hbm, rows_v), ("mgain", mgain_hbm, mgain_ref),
            ("logit", logit_hbm, logit_ref), ("dt", dt_hbm, dt_ref), ("rate", rate_hbm, rate_ref),
            ("x", x_hbm, x_v), ("b", b_hbm.at[gsel, :], b_v), ("c", c_hbm.at[gsel, :], c_v),
            ("tapx", tapx_hbm, tapx_ref), ("tapb", tapb_hbm, tapb_ref), ("tapc", tapc_hbm, tapc_ref),
            ("hgain", hgain_hbm, hgain_ref),
            ("wg", wg_hbm.at[0], wg_v), ("wu", wu_hbm.at[0], wu_v), ("wd", wd_hbm.at[0], wd_v),
            ("z", z_hbm, z_v),
        )
    ):
        loads[name] = pltpu.make_async_copy(src, dst, load_sem.at[i])
        loads[name].start()

    def ready(*names):
        for name in names:
            loads[name].wait()

    ready("routes")
    routes = routes_ref[...]
    row_e = lax.broadcasted_iota(jnp.int32, (EP, tokens), 0)
    hits = [(routes[k : k + 1, :] == row_e).astype(F32) for k in range(2)]
    before = (
        lax.broadcasted_iota(jnp.int32, (tokens, tokens), 0)
        < lax.broadcasted_iota(jnp.int32, (tokens, tokens), 1)
    ).astype(BF16)
    ahead = mm((hits[0] + hits[1]).astype(BF16), before)
    row_s = lax.broadcasted_iota(jnp.int32, (ROWS, tokens), 0)
    hots = []
    for k in range(2):
        rank = jnp.sum(ahead * hits[k], axis=0, keepdims=True).astype(jnp.int32)
        hots.append(row_s == routes[k : k + 1, :] * CAP + rank)
    onehot = (hots[0] | hots[1]).astype(F32).astype(BF16)

    ready("rows", "mgain")
    rows_f = rows_v[...].astype(F32)
    row_scale = lax.rsqrt(jnp.mean(rows_f * rows_f, axis=1, keepdims=True) + ROW_EPS)
    own_cols = rows_v[:, pl.ds(pl.multiple_of(tp * LANES, LANES), LANES)].astype(F32)
    normed = (own_cols * row_scale * mgain_ref[pl.ds(tp, 1), :]).astype(BF16)
    packed = mm(onehot, normed).astype(BF16)
    put(outbox, packed)

    pl.semaphore_wait(barrier, EP - 1 + 3)

    reaches = list(zip(offsets, partners))
    for h in range(2):
        for (dz, dx), tgt in reaches:
            there = seat[(-dz) % NZ, (-dx) % NX]
            if there // (EP // 2) == h:
                rcopy(
                    outbox.at[pl.ds(tgt * UC, UC)],
                    inbox.at[pl.ds(there * UC, UC)],
                    disp_send,
                    disp_recv.at[h],
                    at_ep(tgt),
                ).start()

    ready("x", "b", "c")
    last = pl.ds(L - LANES, LANES)
    rim_pick = (
        lax.broadcasted_iota(jnp.int32, (16, LANES), 0) + (LANES - 16)
        == lax.broadcasted_iota(jnp.int32, (16, LANES), 1)
    ).astype(F32).astype(BF16)
    edge = jnp.concatenate([x_v[:, last], b_v[:, last], c_v[:, last]], axis=0)
    rim_out[...] = mm(rim_pick, edge, (((1,), (1,)), ((), ()))).astype(BF16)
    halo_copy = rcopy(rim_out, rim_in, halo_send, halo_recv, at_ep(lax.rem(ep + 1, EP)))
    halo_copy.start()
    inbox[pl.ds(0, UC)] = outbox[pl.ds(ep * UC, UC)]

    reach = NY // 2
    streams = []
    for q in range(4):
        streams.append((q, 1, reach - q % 2))
        streams.append((q, -1, reach - 1 + q % 2))

    def lane(o, c):
        return lax.rem(y + o + NY, NY) * 2 + c

    def part_of(q):
        return pl.ds(q * quarter, quarter)

    def half_of(h):
        return pl.ds(h * half_rows, half_rows)

    phases = ((0, 3), (1, 2), (4, 7), (5, 6))
    slots, count = {}, 0
    for k in range(8):
        for i in range(streams[k][2]):
            slots[k, i] = count
            count += 1

    def live(p, i):
        return [k for k in phases[p] if i < streams[k][2]]

    def ring(k, i):
        q, s, _ = streams[k]
        blk = xall.at[lane(-s * i, core), part_of(q)]
        return rcopy(blk, blk, ag_send, ag_recv.at[slots[k, i]], to_y(s))

    def ring_recv(k, i):
        q, s, _ = streams[k]
        blk = xall.at[lane(-s * (i + 1), core), part_of(q)]
        return rcopy(blk, blk, ag_send, ag_recv.at[slots[k, i]], to_y(s))

    def cross(o, q):
        blk = xall.at[lane(o, core), part_of(q)]
        return rcopy(blk, blk, d2_send, d2_recv.at[o % NY, q // 2], sibling)

    def cross_half(o, h, c):
        blk = xall.at[lane(o, c), half_of(h)]
        return rcopy(blk, blk, d2_send, d2_recv.at[o % NY, h], sibling)

    def drain(i, p):
        for k in live(p, i):
            q, s, n = streams[k]
            ring_recv(k, i).wait_recv()
            if i + 1 < n:
                ring(k, i + 1).start()
            cross(-s * (i + 1), q).start()

    def expand(*blocks, first=False):
        for o, h in blocks:
            cross_half(o, h, other).wait_recv()
        for o, h in blocks:
            yy = lax.rem(y + o + NY, NY)
            rows = jnp.concatenate([xall[2 * yy, half_of(h), :], xall[2 * yy + 1, half_of(h), :]], axis=1)
            ks = pl.ds(pl.multiple_of(yy * 2 * LANES, 2 * LANES), 2 * LANES)
            for acc, w in ((gate_acc, wg_v), (up_acc, wu_v)):
                prod = mm(rows, w[:, ks], (((1,), (1,)), ((), ())))
                if first:
                    acc[half_of(h), :] = prod
                else:
                    acc[half_of(h), :] += prod

    def own_ready(h):
        count = EP // 2 - 1 + h
        wait_bytes(outbox.at[pl.ds(0, count * UC)], disp_recv.at[h])
        xall[tp, half_of(h), :] = flat(inbox[pl.ds(h * (EP // 2) * UC, EP // 2 * UC)])
        for p in (2 * h, 2 * h + 1):
            for k in live(p, 0):
                ring(k, 0).start()
        cross_half(0, h, core).start()

    ready("logit", "dt", "rate")
    logit = logit_ref[...]
    share = jax.nn.sigmoid(logit[0:1, :] - logit[1:2, :])
    weighted = jnp.where(hots[0], share, jnp.where(hots[1], jax.nn.sigmoid(logit[1:2, :] - logit[0:1, :]), 0.0))
    weighted = jnp.transpose(weighted)
    coarse = weighted.astype(BF16)
    pick[0] = coarse
    pick[1] = (weighted - coarse.astype(F32)).astype(BF16)

    dt = dt_ref[...]
    step = jnp.maximum(dt, 0.0) + jnp.log1p(jnp.exp(-jnp.abs(dt)))
    eye = lax.broadcasted_iota(jnp.int32, (HH, HH), 0) == lax.broadcasted_iota(jnp.int32, (HH, HH), 1)
    rate = jnp.sum(jnp.where(eye, rate_ref[...], 0.0), axis=1, keepdims=True)
    logd = -step * rate
    upper = (
        lax.broadcasted_iota(jnp.int32, (LANES, LANES), 0)
        <= lax.broadcasted_iota(jnp.int32, (LANES, LANES), 1)
    ).astype(F32)
    pieces, carry = [], jnp.zeros((HH, 1), F32)
    for k in range(NB):
        piece = (
            jnp.dot(
                logd[:, k * LANES : (k + 1) * LANES], upper, precision=HIGHEST, preferred_element_type=F32
            )
            + carry
        )
        carry = piece[:, LANES - 1 : LANES]
        pieces.append(piece)
    cum = jnp.concatenate(pieces, axis=1)
    total = carry
    cum_v[pl.ds(0, HH), :] = cum
    tall = jnp.concatenate([cum, jnp.zeros((8 - HH, L), F32)], axis=0)
    colv[...] = jnp.transpose(tall)

    started = (ep > 0).astype(F32)

    def conv(cur, rim, taps):
        joined = jnp.concatenate([rim.astype(F32) * started, cur.astype(F32)], axis=1)
        out = taps[:, 3:4] * joined[:, LANES:]
        for k in range(3):
            out = out + taps[:, k : k + 1] * pltpu.roll(joined, 3 - k, 1)[:, LANES:]
        return out * jax.nn.sigmoid(out)

    kept = {}

    def taps_part():
        halo_copy.wait_recv()
        halo[...] = mm(rim_in[...], rim_pick, (((0,), (0,)), ((), ()))).astype(BF16)
        ready("tapx", "tapb", "tapc", "hgain")
        kept["bc"] = jnp.transpose(jnp.concatenate([tapb_ref[:, gsel], tapc_ref[:, gsel]], axis=0))
        kept["x"] = jnp.transpose(
            jnp.concatenate([tapx_ref[...], hgain_ref[...], jnp.zeros((3, VR), F32)], axis=0)
        )
        bc_v[...] = conv(b_v[...], halo[pl.ds(VR, NSTATE), :], kept["bc"][:, :4]).astype(BF16)

    def value_part(heads):
        tail = jnp.exp(total - cum)
        for h in heads:
            rows_h = pl.ds(h * HD, HD)
            xc = conv(x_v[rows_h, :], halo[rows_h, :], kept["x"][h * HD : (h + 1) * HD, :4])
            xs = xc * step[h : h + 1, :]
            xs_v[rows_h, :] = xs.astype(BF16)
            yloc[rows_h, :] = xs * tail[h : h + 1, :]

    own_ready(0)
    ready("wg", "wu")
    expand((0, 0), first=True)
    own_ready(1)

    def send_part():
        state = mm(yloc[...].astype(BF16), bc_v[...], (((1,), (1,)), ((), ())))
        hi = total.astype(BF16).astype(F32)
        mid = (total - hi).astype(BF16).astype(F32)
        low = total - hi - mid
        r8 = lax.broadcasted_iota(jnp.int32, (8, LANES), 0)
        for u in range(EP):
            h = u * U // HD
            decay = jnp.where(
                r8 == 0,
                hi[h : h + 1],
                jnp.where(r8 == 1, mid[h : h + 1], jnp.where(r8 == 2, low[h : h + 1], 0.0)),
            )
            extra = [state[u * U : (u + 1) * U], decay]
            if UR > U + 8:
                extra.append(jnp.zeros((UR - U - 8, LANES), F32))
            sout[u] = jnp.concatenate(extra, axis=0).astype(BF16)

        @pl.loop(1, EP)
        def _(d):
            tgt = lax.rem(ep + d, EP)
            rcopy(sout.at[tgt], sin.at[ep], st_send, st_recv, at_ep(tgt)).start()

        sin[ep] = sout[ep]

    def gram_part():
        c_conv = conv(c_v[...], halo[pl.ds(VR + NSTATE, NSTATE), :], kept["bc"][:, 4:]).astype(BF16)
        cc_v[...] = c_conv
        gram_v[...] = mm(bc_v[...], c_conv, (((0,), (0,)), ((), ())))

    def local_part(heads):
        diag = lax.broadcasted_iota(jnp.int32, (LANES, LANES), 0) <= lax.broadcasted_iota(
            jnp.int32, (LANES, LANES), 1
        )
        for h in heads:
            for j in range(NB):
                at = cum_v[h : h + 1, j * LANES : (j + 1) * LANES]
                pieces = []
                for i in range(j + 1):
                    gap = at - colv[i * LANES : (i + 1) * LANES, h : h + 1]
                    if i == j:
                        gap = jnp.where(diag, gap, -jnp.inf)
                    g = gram_v[i * LANES : (i + 1) * LANES, j * LANES : (j + 1) * LANES]
                    pieces.append((g * jnp.exp(gap)).astype(BF16))
                weights = jnp.concatenate(pieces, axis=0) if j else pieces[0]
                rows_h = pl.ds(h * HD, HD)
                yloc[rows_h, j * LANES : (j + 1) * LANES] = mm(
                    xs_v[rows_h, : (j + 1) * LANES], weights
                )

    def prefix_part():
        wait_bytes(sout.at[pl.ds(0, EP - 1)], st_recv)
        held = jnp.zeros((U, LANES), F32)
        for e in range(EP):
            hout[e] = held
            blk = sin[e].astype(F32)
            keep = jnp.exp(blk[U : U + 1] + blk[U + 1 : U + 2] + blk[U + 2 : U + 3])
            held = keep * held + blk[:U]

        @pl.loop(1, EP)
        def _(d):
            tgt = lax.rem(ep + d, EP)
            rcopy(hout.at[tgt], hin.at[ep], hb_send, hb_recv, at_ep(tgt)).start()

        hin[ep] = hout[ep]

    def final_part():
        ready("z")
        wait_bytes(hout.at[pl.ds(0, EP - 1)], hb_recv)
        before = hin[...].reshape(VR, LANES).astype(BF16)
        for h in range(HH):
            rows_h = pl.ds(h * HD, HD)
            carried = mm(before[h * HD : (h + 1) * HD], cc_v[...]) * jnp.exp(cum_v[h : h + 1, :])
            z = z_v[rows_h, :].astype(F32)
            gated = (yloc[rows_h, :] + carried) * (z * jax.nn.sigmoid(z))
            scale = lax.rsqrt(jnp.mean(gated * gated, axis=0, keepdims=True) + HEAD_EPS)
            gain = kept["x"][h * HD : (h + 1) * HD, 4:5]
            mixed_ref[rows_h, :] = (gated * scale * gain).astype(BF16)

    pieces = [
        taps_part,
        lambda: value_part(range(HH // 2)),
        lambda: value_part(range(HH // 2, HH)),
        send_part,
        gram_part,
        lambda: local_part([0]),
        lambda: local_part([1]),
        lambda: local_part(range(2, HH)),
    ]

    far = reach - 1
    for i in range(far):
        for p in range(4):
            drain(i, p)
            if (i, p) == (0, 1):
                expand((0, 1), first=True)
            if p == 3:
                expand((i + 1, 0))
            elif i:
                expand(((-i, i, -i)[p], (0, 1, 1)[p]))
            if (i or p > 1) and pieces:
                pieces.pop(0)()
    for piece in pieces:
        piece()
    drain(far, 0)
    if far:
        expand((-far, 0), (far, 1))
    drain(far, 1)
    drain(far, 2)
    drain(far, 3)

    ready("wd")

    def activate(h):
        gate = gate_acc[half_of(h), :]
        hid[half_of(h), :] = (gate * jax.nn.sigmoid(gate) * up_acc[half_of(h), :]).astype(BF16)

    def swap(o, h):
        return rcopy(
            part.at[o % NY, other, half_of(h)], sib.at[o % NY, half_of(h)], ps_send, ps_recv.at[o % NY, h], sibling
        )

    def project(*blocks):
        prods = []
        for o, h in blocks:
            yy = lax.rem(y + o + NY, NY)
            cols = pl.ds(pl.multiple_of(yy * 2 * LANES, 2 * LANES), 2 * LANES)
            prods.append(mm(hid[half_of(h), :], wd_v[:, cols]).astype(BF16))
        for (o, h), prod in zip(blocks, prods):
            part[o % NY, 0, half_of(h), :] = prod[:, :LANES]
            part[o % NY, 1, half_of(h), :] = prod[:, LANES:]
        for o, h in blocks:
            swap(o, h).start()

    swapped = set()

    def pair_sum(o, q):
        at = (o % NY, q // 2)
        if at not in swapped:
            swap(*at).wait_recv()
            swapped.add(at)
        mine = part[o % NY, core, part_of(q), :].astype(F32)
        return mine + sib[o % NY, part_of(q), :].astype(F32)

    def push(k, i):
        j = slots[k, i]
        return rcopy(tosend.at[j], arrived.at[j], rs_send, rs_recv.at[j], to_y(streams[k][1]))

    def came(k, i):
        push(k, i).wait_recv()
        return arrived[slots[k, i]].astype(F32)

    def feed(k, i):
        q, s, n = streams[k]
        value = pair_sum(s * (n - i), q)
        if i:
            value = value + came(k, i - 1)
        tosend[slots[k, i]] = value.astype(BF16)
        push(k, i).start()

    def feed_all(p, i):
        for k in live(p, i):
            feed(k, i)

    def sides(i, h):
        m = reach - 1 - i
        return [] if m < 0 else [(o, h) for o in sorted({-m, m})]

    expand((reach, 0))
    activate(0)
    project((reach, 0))
    expand(*([(-far, 1)] if far else []), (reach, 1))
    activate(1)
    first, second = sides(0, 0), sides(0, 1)
    project((reach, 1), *first[:1])
    feed_all(0, 0)
    project(*first[1:], *second[:1])
    feed_all(2, 0)
    project(*second[1:])
    feed_all(1, 0)
    project(*sides(1, 0))
    feed_all(3, 0)
    for i in range(1, reach):
        for at, p in enumerate((0, 2, 1, 3)):
            feed_all(p, i)
            coming = ([], sides(i, 1), [], sides(i + 1, 0))[at]
            if coming:
                project(*coming)
            if (i, at) == (1, 2 if far > 1 else 0):
                prefix_part()
    units = quarter // QUAD
    for h in range(2):
        for q in (2 * h, 2 * h + 1):
            value = pair_sum(0, q)
            for k in (2 * q, 2 * q + 1):
                if streams[k][2] > 0:
                    value = value + came(k, streams[k][2] - 1)
            put(rout.at[pl.ds(q * units, units)], value.astype(BF16))
        for offset, tgt in reaches:
            if seat[offset] // (EP // 2) == h:
                rcopy(
                    rout.at[pl.ds(seat[offset] * UC, UC)], rin.at[pl.ds(ep * UC, UC)], rt_send, rt_recv, at_ep(tgt)
                ).start()
    rin[pl.ds(ep * UC, UC)] = rout[pl.ds(0, UC)]

    final_part()
    wait_bytes(outbox.at[pl.ds(0, (EP - 1) * UC)], disp_send)
    halo_copy.wait_send()
    wait_bytes(sout.at[pl.ds(0, EP - 1)], st_send)
    wait_bytes(hout.at[pl.ds(0, EP - 1)], hb_send)
    wait_bytes(xall.at[pl.ds(0, NY - 1)], ag_send)
    wait_bytes(xall.at[pl.ds(0, NY)], d2_send)
    wait_bytes(sib, ps_send)
    wait_bytes(tosend, rs_send)

    wait_bytes(rout.at[pl.ds(0, (EP - 1) * UC)], rt_recv)
    back = flat(rin[...])
    moe_ref[...] = (mm(pick[0], back) + mm(pick[1], back)).astype(BF16)
    wait_bytes(rout.at[pl.ds(0, (EP - 1) * UC)], rt_send)


def place_body(mixed_ref, moe_ref, mixed_out, moe_out, sem):
    copies = [
        pltpu.make_async_copy(mixed_ref, mixed_out, sem.at[0]),
        pltpu.make_async_copy(moe_ref, moe_out, sem.at[1]),
    ]
    for copy in copies:
        copy.start()
    for copy in copies:
        copy.wait()


def on_device(EP, TP, *args):
    (x_in, z_in, dt_raw, decay_rate, b_in, c_in, conv_x, conv_b, conv_c, head_gain,
     moe_rows, moe_gain, routes, route_logit, w_gate, w_up, w_down) = args
    tokens, features = moe_rows.shape
    CAP = 2 * tokens * routes.shape[1] // EP
    VR, L = x_in.shape
    HH = dt_raw.shape[0]
    FD = w_gate.shape[2]
    flipped = functools.partial(jnp.swapaxes, axis1=-2, axis2=-1)
    NY = TP // 2
    ROWS = EP * CAP
    U = VR // EP
    UR = -(-(U + 8) // 16) * 16
    cfg = dict(EP=EP, TP=TP, CAP=CAP, L=L, HH=HH)
    hbm, vmem = (pl.BlockSpec(memory_space=m) for m in (pltpu.HBM, pltpu.VMEM))
    dma = pltpu.SemaphoreType.DMA
    units = (ROWS // QUAD, QUAD, LANES)
    block = (ROWS, LANES)
    piece = (ROWS // 4, LANES)
    hops = 4 * (2 * (NY // 2) - 1)
    scratch = [
        pltpu.VMEM((HH, L), F32), pltpu.VMEM((1, HH), F32),
        pltpu.VMEM((4, VR), F32), pltpu.VMEM((4, conv_b.shape[0]), F32), pltpu.VMEM((4, conv_b.shape[0]), F32),
        pltpu.VMEM((1, VR), F32), pltpu.VMEM((TP, features // TP), F32),
        pltpu.VMEM((2, tokens), jnp.int32), pltpu.VMEM((2, tokens), F32),
        pltpu.VMEM((VR, L), BF16), pltpu.VMEM((VR, L), BF16),
        pltpu.VMEM((NSTATE, L), BF16), pltpu.VMEM((NSTATE, L), BF16),
        pltpu.VMEM((tokens, features), BF16),
        pltpu.VMEM((FD, features), BF16), pltpu.VMEM((FD, features), BF16), pltpu.VMEM((FD, features), BF16),
        pltpu.VMEM((VR + 2 * NSTATE, LANES), BF16),
        pltpu.VMEM((16, VR + 2 * NSTATE), BF16), pltpu.VMEM((16, VR + 2 * NSTATE), BF16),
        pltpu.VMEM((2, tokens, ROWS), BF16),
        pltpu.VMEM(units, BF16), pltpu.VMEM(units, BF16), pltpu.VMEM((TP,) + block, BF16),
        pltpu.VMEM((ROWS, FD), F32), pltpu.VMEM((ROWS, FD), F32), pltpu.VMEM((ROWS, FD), BF16),
        pltpu.VMEM((NY, 2) + block, BF16), pltpu.VMEM((NY,) + block, BF16),
        pltpu.VMEM((hops,) + piece, BF16), pltpu.VMEM((hops,) + piece, BF16),
        pltpu.VMEM(units, BF16), pltpu.VMEM(units, BF16),
        pltpu.VMEM((VR, L), BF16), pltpu.VMEM((NSTATE, L), BF16), pltpu.VMEM((NSTATE, L), BF16),
        pltpu.VMEM((L, L), F32), pltpu.VMEM((8, L), F32), pltpu.VMEM((L, 8), F32), pltpu.VMEM((VR, L), F32),
        pltpu.VMEM((EP, UR, LANES), BF16), pltpu.VMEM((EP, UR, LANES), BF16),
        pltpu.VMEM((EP, U, LANES), F32), pltpu.VMEM((EP, U, LANES), F32),
        dma((17,)), dma, dma, dma, dma((2,)), dma, dma, dma, dma,
        dma, dma((hops,)), dma, dma((NY, 2)), dma, dma((NY, 2)), dma, dma((hops,)), dma, dma,
    ]
    mixed, moe = pl.pallas_call(
        functools.partial(kernel_body, cfg),
        name="mixer_and_experts",
        out_shape=(
            pltpu.VMEM((VR, L), BF16),
            pltpu.VMEM((tokens, features // TP), BF16),
        ),
        in_specs=[hbm] * 17,
        out_specs=(vmem, vmem),
        scratch_shapes=scratch,
        compiler_params=pltpu.CompilerParams(
            collective_id=0, has_side_effects=True, vmem_limit_bytes=60 * 1024 * 1024
        ),
    )(
        x_in, z_in, dt_raw, decay_rate.reshape(1, HH), b_in, c_in, flipped(conv_x), flipped(conv_b), flipped(conv_c),
        head_gain.reshape(1, VR), moe_rows, moe_gain.reshape(TP, features // TP),
        flipped(routes), flipped(route_logit), flipped(w_gate), flipped(w_up), w_down,
    )
    mixed, moe = pl.pallas_call(
        place_body,
        name="place",
        out_shape=(jax.ShapeDtypeStruct(mixed.shape, BF16), jax.ShapeDtypeStruct(moe.shape, BF16)),
        in_specs=[vmem, vmem],
        out_specs=(hbm, hbm),
        scratch_shapes=[dma((2,))],
    )(*(pltpu.with_memory_space_constraint(o, pltpu.VMEM) for o in (mixed, moe)))
    return mixed, flipped(moe)


def solution(mesh):
    EP, TP = mesh.shape["ep"], mesh.shape["tp"]
    in_specs = (
        P("tp", "ep"), P("tp", "ep"), P("tp", "ep"), P("tp"), P(None, "ep"), P(None, "ep"),
        P("tp", None), P(), P(), P("tp"), P("ep", None), P(), P("ep", None), P("ep", None),
        P("ep", None, "tp"), P("ep", None, "tp"), P("ep", "tp", None),
    )
    return jax.shard_map(
        functools.partial(on_device, EP, TP),
        mesh=mesh,
        in_specs=in_specs,
        out_specs=(P("tp", "ep"), P("tp", "ep")),
        check_vma=False,
    )
```

```python
import functools

import jax
import jax.numpy as jnp
from jax import lax
from jax.experimental import pallas as pl
from jax.experimental.pallas import tpu as pltpu
from jax.sharding import PartitionSpec as P

F32 = jnp.float32
BF16 = jnp.bfloat16
MESH = pl.DeviceIdType.MESH
HIGHEST = lax.Precision.HIGHEST
GROUPS = 2
NSTATE = 128
LANES = 128
QUAD = 4
ROW_EPS = 0.1
HEAD_EPS = 1.0


def mm(a, b, dims=(((1,), (0,)), ((), ()))):
    return lax.dot_general(a, b, dims, preferred_element_type=F32)


def kernel_body(
    cfg,
    x_hbm, z_hbm, dt_hbm, rate_hbm, b_hbm, c_hbm, tapx_hbm, tapb_hbm, tapc_hbm, hgain_hbm,
    rows_hbm, mgain_hbm, routes_hbm, logit_hbm, wg_hbm, wu_hbm, wd_hbm,
    mixed_ref, moe_ref,
    dt_ref, rate_ref, tapx_ref, tapb_ref, tapc_ref, hgain_ref, mgain_ref, routes_ref, logit_ref,
    x_v, z_v, b_v, c_v, rows_v, wg_v, wu_v, wd_v, halo, rim_out, rim_in, pick, outbox, inbox, xall,
    gate_acc, up_acc, hid, part, sib, tosend, arrived, rout, rin,
    xs_v, bc_v, cc_v, gram_v, cum_v, colv, yloc, sout, sin, hout, hin,
    load_sem, halo_send, halo_recv, disp_send, disp_recv, st_send, st_recv, hb_send, hb_recv,
    ag_send, ag_recv, d2_send, d2_recv, ps_send, ps_recv, rs_send, rs_recv, rt_send, rt_recv,
):
    EP, TP, CAP, L, HH = cfg["EP"], cfg["TP"], cfg["CAP"], cfg["L"], cfg["HH"]
    NY = TP // 2
    UC = CAP // QUAD
    ROWS = EP * CAP
    half_rows, quarter = ROWS // 2, ROWS // 4
    tokens = rows_v.shape[0]
    VR = x_v.shape[0]
    HD = VR // HH
    NB = L // LANES
    U = VR // EP
    UR = sout.shape[1]
    ep, tp = lax.axis_index("ep"), lax.axis_index("tp")
    y, core = lax.div(tp, 2), lax.rem(tp, 2)
    other = 1 - core
    group = lax.div(tp, TP // GROUPS)

    NX = min(4, EP)
    NZ = EP // NX
    z_at, x_at = lax.div(ep, NX), lax.rem(ep, NX)

    def hops(offset):
        dz, dx = offset
        return min(dz, NZ - dz) + min(dx, NX - dx)

    ranked = sorted(((dz, dx) for dz in range(NZ) for dx in range(NX)), key=hops)
    seat = {offset: i for i, offset in enumerate(ranked)}
    offsets = ranked[:0:-1]
    partners = [lax.rem(z_at + dz, NZ) * NX + lax.rem(x_at + dx, NX) for dz, dx in offsets]

    def at_ep(index):
        return {"ep": index, "tp": tp}

    def to_y(s):
        return {"ep": ep, "tp": lax.rem(y + s + NY, NY) * 2 + core}

    sibling = {"ep": ep, "tp": y * 2 + other}

    def rcopy(src, dst, ssem, rsem, dev):
        return pltpu.make_async_remote_copy(
            src_ref=src, dst_ref=dst, send_sem=ssem, recv_sem=rsem, device_id=dev, device_id_type=MESH
        )

    def flat(block):
        return block.reshape(block.shape[0] * QUAD, LANES)

    def put(ref, value):
        ref[...] = value.reshape(value.shape[0] // QUAD, QUAD, LANES)

    def wait_bytes(ref, sem):
        pltpu.make_async_copy(ref, ref, sem).wait()

    barrier = pltpu.get_barrier_semaphore()

    for tgt in partners:
        pl.semaphore_signal(barrier, inc=1, device_id=at_ep(tgt), device_id_type=MESH)

    for dev in (to_y(1), to_y(-1), sibling):
        pl.semaphore_signal(barrier, inc=1, device_id=dev, device_id_type=MESH)

    gsel = pl.ds(pl.multiple_of(group * NSTATE, NSTATE), NSTATE)
    loads = {}
    for i, (name, src, dst) in enumerate(
        (
            ("routes", routes_hbm, routes_ref), ("rows", rows_hbm, rows_v), ("mgain", mgain_hbm, mgain_ref),
            ("logit", logit_hbm, logit_ref), ("dt", dt_hbm, dt_ref), ("rate", rate_hbm, rate_ref),
            ("x", x_hbm, x_v), ("b", b_hbm.at[gsel, :], b_v), ("c", c_hbm.at[gsel, :], c_v),
            ("tapx", tapx_hbm, tapx_ref), ("tapb", tapb_hbm, tapb_ref), ("tapc", tapc_hbm, tapc_ref),
            ("hgain", hgain_hbm, hgain_ref),
            ("wg", wg_hbm.at[0], wg_v), ("wu", wu_hbm.at[0], wu_v), ("wd", wd_hbm.at[0], wd_v),
            ("z", z_hbm, z_v),
        )
    ):
        loads[name] = pltpu.make_async_copy(src, dst, load_sem.at[i])
        loads[name].start()

    def ready(*names):
        for name in names:
            loads[name].wait()

    ready("routes")
    routes = routes_ref[...]
    row_e = lax.broadcasted_iota(jnp.int32, (EP, tokens), 0)
    hits = [(routes[k : k + 1, :] == row_e).astype(F32) for k in range(2)]
    before = (
        lax.broadcasted_iota(jnp.int32, (tokens, tokens), 0)
        < lax.broadcasted_iota(jnp.int32, (tokens, tokens), 1)
    ).astype(BF16)
    ahead = mm((hits[0] + hits[1]).astype(BF16), before)
    row_s = lax.broadcasted_iota(jnp.int32, (ROWS, tokens), 0)
    hots = []
    for k in range(2):
        rank = jnp.sum(ahead * hits[k], axis=0, keepdims=True).astype(jnp.int32)
        hots.append(row_s == routes[k : k + 1, :] * CAP + rank)
    onehot = (hots[0] | hots[1]).astype(F32).astype(BF16)

    ready("rows", "mgain")
    rows_f = rows_v[...].astype(F32)
    row_scale = lax.rsqrt(jnp.mean(rows_f * rows_f, axis=1, keepdims=True) + ROW_EPS)
    own_cols = rows_v[:, pl.ds(pl.multiple_of(tp * LANES, LANES), LANES)].astype(F32)
    normed = (own_cols * row_scale * mgain_ref[pl.ds(tp, 1), :]).astype(BF16)
    packed = mm(onehot, normed).astype(BF16)
    put(outbox, packed)

    pl.semaphore_wait(barrier, EP - 1 + 3)

    reaches = list(zip(offsets, partners))
    for h in range(2):
        for (dz, dx), tgt in reaches:
            there = seat[(-dz) % NZ, (-dx) % NX]
            if there // (EP // 2) == h:
                rcopy(
                    outbox.at[pl.ds(tgt * UC, UC)],
                    inbox.at[pl.ds(there * UC, UC)],
                    disp_send,
                    disp_recv.at[h],
                    at_ep(tgt),
                ).start()

    ready("x", "b", "c")
    last = pl.ds(L - LANES, LANES)
    rim_pick = (
        lax.broadcasted_iota(jnp.int32, (16, LANES), 0) + (LANES - 16)
        == lax.broadcasted_iota(jnp.int32, (16, LANES), 1)
    ).astype(F32).astype(BF16)
    edge = jnp.concatenate([x_v[:, last], b_v[:, last], c_v[:, last]], axis=0)
    rim_out[...] = mm(rim_pick, edge, (((1,), (1,)), ((), ()))).astype(BF16)
    halo_copy = rcopy(rim_out, rim_in, halo_send, halo_recv, at_ep(lax.rem(ep + 1, EP)))
    halo_copy.start()
    inbox[pl.ds(0, UC)] = outbox[pl.ds(ep * UC, UC)]

    reach = NY // 2
    streams = []
    for q in range(4):
        streams.append((q, 1, reach - q % 2))
        streams.append((q, -1, reach - 1 + q % 2))

    def lane(o, c):
        return lax.rem(y + o + NY, NY) * 2 + c

    def part_of(q):
        return pl.ds(q * quarter, quarter)

    def half_of(h):
        return pl.ds(h * half_rows, half_rows)

    phases = ((0, 3), (1, 2), (4, 7), (5, 6))
    slots, count = {}, 0
    for k in range(8):
        for i in range(streams[k][2]):
            slots[k, i] = count
            count += 1

    def live(p, i):
        return [k for k in phases[p] if i < streams[k][2]]

    pair_at = {}
    for p in range(4):
        for i in range(reach):
            if live(p, i):
                pair_at[p, i] = len(pair_at)
    phase_of = {k: p for p in range(4) for k in phases[p]}

    def pair_index(k, i):
        return pair_at[phase_of[k], i]

    def ring(k, i):
        q, s, _ = streams[k]
        blk = xall.at[lane(-s * i, core), part_of(q)]
        return rcopy(blk, blk, ag_send, ag_recv.at[pair_index(k, i)], to_y(s))

    def cross(o, q):
        blk = xall.at[lane(o, core), part_of(q)]
        return rcopy(blk, blk, d2_send, d2_recv.at[o % NY, q // 2], sibling)

    def cross_half(o, h, c):
        blk = xall.at[lane(o, c), half_of(h)]
        return rcopy(blk, blk, d2_send, d2_recv.at[o % NY, h], sibling)

    def drain(i, p):
        if live(p, i):
            wait_bytes(xall.at[0, half_of(0)], ag_recv.at[pair_at[p, i]])
        for k in live(p, i):
            if i + 1 < streams[k][2]:
                ring(k, i + 1).start()
        for k in live(p, i):
            q, s, _ = streams[k]
            cross(-s * (i + 1), q).start()

    def expand(*blocks, first=False):
        for o, h in blocks:
            cross_half(o, h, other).wait_recv()
        for o, h in blocks:
            yy = lax.rem(y + o + NY, NY)
            rows = jnp.concatenate([xall[2 * yy, half_of(h), :], xall[2 * yy + 1, half_of(h), :]], axis=1)
            ks = pl.ds(pl.multiple_of(yy * 2 * LANES, 2 * LANES), 2 * LANES)
            for acc, w in ((gate_acc, wg_v), (up_acc, wu_v)):
                prod = mm(rows, w[:, ks], (((1,), (1,)), ((), ())))
                if first:
                    acc[half_of(h), :] = prod
                else:
                    acc[half_of(h), :] += prod

    def own_ready(h):
        count = EP // 2 - 1 + h
        wait_bytes(outbox.at[pl.ds(0, count * UC)], disp_recv.at[h])
        xall[tp, half_of(h), :] = flat(inbox[pl.ds(h * (EP // 2) * UC, EP // 2 * UC)])
        for p in (2 * h, 2 * h + 1):
            for k in live(p, 0):
                ring(k, 0).start()
        cross_half(0, h, core).start()

    ready("logit", "dt", "rate")
    logit = logit_ref[...]
    share = jax.nn.sigmoid(logit[0:1, :] - logit[1:2, :])
    weighted = jnp.where(hots[0], share, jnp.where(hots[1], jax.nn.sigmoid(logit[1:2, :] - logit[0:1, :]), 0.0))
    weighted = jnp.transpose(weighted)
    coarse = weighted.astype(BF16)
    pick[0] = coarse
    pick[1] = (weighted - coarse.astype(F32)).astype(BF16)

    dt = dt_ref[...]
    step = jnp.maximum(dt, 0.0) + jnp.log1p(jnp.exp(-jnp.abs(dt)))
    eye = lax.broadcasted_iota(jnp.int32, (HH, HH), 0) == lax.broadcasted_iota(jnp.int32, (HH, HH), 1)
    rate = jnp.sum(jnp.where(eye, rate_ref[...], 0.0), axis=1, keepdims=True)
    logd = -step * rate
    upper = (
        lax.broadcasted_iota(jnp.int32, (LANES, LANES), 0)
        <= lax.broadcasted_iota(jnp.int32, (LANES, LANES), 1)
    ).astype(F32)
    pieces, carry = [], jnp.zeros((HH, 1), F32)
    for k in range(NB):
        piece = (
            jnp.dot(
                logd[:, k * LANES : (k + 1) * LANES], upper, precision=HIGHEST, preferred_element_type=F32
            )
            + carry
        )
        carry = piece[:, LANES - 1 : LANES]
        pieces.append(piece)
    cum = jnp.concatenate(pieces, axis=1)
    total = carry
    cum_v[pl.ds(0, HH), :] = cum
    tall = jnp.concatenate([cum, jnp.zeros((8 - HH, L), F32)], axis=0)
    colv[...] = jnp.transpose(tall)

    started = (ep > 0).astype(F32)

    def conv(cur, rim, taps):
        joined = jnp.concatenate([rim.astype(F32) * started, cur.astype(F32)], axis=1)
        out = taps[:, 3:4] * joined[:, LANES:]
        for k in range(3):
            out = out + taps[:, k : k + 1] * pltpu.roll(joined, 3 - k, 1)[:, LANES:]
        return out * jax.nn.sigmoid(out)

    kept = {}

    def taps_part():
        halo_copy.wait_recv()
        halo[...] = mm(rim_in[...], rim_pick, (((0,), (0,)), ((), ()))).astype(BF16)
        ready("tapx", "tapb", "tapc", "hgain")
        kept["bc"] = jnp.transpose(jnp.concatenate([tapb_ref[:, gsel], tapc_ref[:, gsel]], axis=0))
        kept["x"] = jnp.transpose(
            jnp.concatenate([tapx_ref[...], hgain_ref[...], jnp.zeros((3, VR), F32)], axis=0)
        )
        bc_v[...] = conv(b_v[...], halo[pl.ds(VR, NSTATE), :], kept["bc"][:, :4]).astype(BF16)

    def value_part(heads):
        tail = jnp.exp(total - cum)
        for h in heads:
            rows_h = pl.ds(h * HD, HD)
            xc = conv(x_v[rows_h, :], halo[rows_h, :], kept["x"][h * HD : (h + 1) * HD, :4])
            xs = xc * step[h : h + 1, :]
            xs_v[rows_h, :] = xs.astype(BF16)
            yloc[rows_h, :] = xs * tail[h : h + 1, :]

    own_ready(0)
    ready("wg", "wu")
    expand((0, 0), first=True)
    own_ready(1)

    def send_part():
        state = mm(yloc[...].astype(BF16), bc_v[...], (((1,), (1,)), ((), ())))
        hi = total.astype(BF16).astype(F32)
        mid = (total - hi).astype(BF16).astype(F32)
        low = total - hi - mid
        r8 = lax.broadcasted_iota(jnp.int32, (8, LANES), 0)
        for u in range(EP):
            h = u * U // HD
            decay = jnp.where(
                r8 == 0,
                hi[h : h + 1],
                jnp.where(r8 == 1, mid[h : h + 1], jnp.where(r8 == 2, low[h : h + 1], 0.0)),
            )
            extra = [state[u * U : (u + 1) * U], decay]
            if UR > U + 8:
                extra.append(jnp.zeros((UR - U - 8, LANES), F32))
            sout[u] = jnp.concatenate(extra, axis=0).astype(BF16)

        for tgt in partners:
            rcopy(sout.at[tgt], sin.at[ep], st_send, st_recv, at_ep(tgt)).start()

        sin[ep] = sout[ep]

    def gram_part():
        c_conv = conv(c_v[...], halo[pl.ds(VR + NSTATE, NSTATE), :], kept["bc"][:, 4:]).astype(BF16)
        cc_v[...] = c_conv
        gram_v[...] = mm(bc_v[...], c_conv, (((0,), (0,)), ((), ())))

    def local_part(heads):
        diag = lax.broadcasted_iota(jnp.int32, (LANES, LANES), 0) <= lax.broadcasted_iota(
            jnp.int32, (LANES, LANES), 1
        )
        for h in heads:
            for j in range(NB):
                at = cum_v[h : h + 1, j * LANES : (j + 1) * LANES]
                pieces = []
                for i in range(j + 1):
                    gap = at - colv[i * LANES : (i + 1) * LANES, h : h + 1]
                    if i == j:
                        gap = jnp.where(diag, gap, -jnp.inf)
                    g = gram_v[i * LANES : (i + 1) * LANES, j * LANES : (j + 1) * LANES]
                    pieces.append((g * jnp.exp(gap)).astype(BF16))
                weights = jnp.concatenate(pieces, axis=0) if j else pieces[0]
                rows_h = pl.ds(h * HD, HD)
                yloc[rows_h, j * LANES : (j + 1) * LANES] = mm(
                    xs_v[rows_h, : (j + 1) * LANES], weights
                )

    def prefix_part():
        wait_bytes(sout.at[pl.ds(0, EP - 1)], st_recv)
        held = jnp.zeros((U, LANES), F32)
        for e in range(EP):
            hout[e] = held
            blk = sin[e].astype(F32)
            keep = jnp.exp(blk[U : U + 1] + blk[U + 1 : U + 2] + blk[U + 2 : U + 3])
            held = keep * held + blk[:U]

        for tgt in partners:
            rcopy(hout.at[tgt], hin.at[ep], hb_send, hb_recv, at_ep(tgt)).start()

        hin[ep] = hout[ep]

    def final_part():
        ready("z")
        wait_bytes(hout.at[pl.ds(0, EP - 1)], hb_recv)
        before = hin[...].reshape(VR, LANES).astype(BF16)
        for h in range(HH):
            rows_h = pl.ds(h * HD, HD)
            carried = mm(before[h * HD : (h + 1) * HD], cc_v[...]) * jnp.exp(cum_v[h : h + 1, :])
            z = z_v[rows_h, :].astype(F32)
            gated = (yloc[rows_h, :] + carried) * (z * jax.nn.sigmoid(z))
            scale = lax.rsqrt(jnp.mean(gated * gated, axis=0, keepdims=True) + HEAD_EPS)
            gain = kept["x"][h * HD : (h + 1) * HD, 4:5]
            mixed_ref[rows_h, :] = (gated * scale * gain).astype(BF16)

    pieces = [
        taps_part,
        lambda: value_part(range(HH // 2)),
        lambda: value_part(range(HH // 2, HH)),
        send_part,
    ]
    later = [gram_part] + [functools.partial(local_part, [h]) for h in range(HH)]

    far = reach - 1
    for i in range(far):
        for p in range(4):
            drain(i, p)
            if (i, p) == (0, 1):
                expand((0, 1), first=True)
            if p == 3:
                expand((i + 1, 0))
            elif i:
                expand(((-i, i, -i)[p], (0, 1, 1)[p]))
            if (i or p > 1) and pieces:
                pieces.pop(0)()
    for piece in pieces:
        piece()
    drain(far, 0)
    if far:
        expand((-far, 0), (far, 1))
    drain(far, 1)
    drain(far, 2)
    drain(far, 3)

    ready("wd")

    def activate(h):
        gate = gate_acc[half_of(h), :]
        hid[half_of(h), :] = (gate * jax.nn.sigmoid(gate) * up_acc[half_of(h), :]).astype(BF16)

    def swap(o, h):
        return rcopy(
            part.at[o % NY, other, half_of(h)], sib.at[o % NY, half_of(h)], ps_send, ps_recv.at[o % NY, h], sibling
        )

    def project(*blocks):
        prods = []
        for o, h in blocks:
            yy = lax.rem(y + o + NY, NY)
            cols = pl.ds(pl.multiple_of(yy * 2 * LANES, 2 * LANES), 2 * LANES)
            prods.append(mm(hid[half_of(h), :], wd_v[:, cols]).astype(BF16))
        for (o, h), prod in zip(blocks, prods):
            part[o % NY, 0, half_of(h), :] = prod[:, :LANES]
            part[o % NY, 1, half_of(h), :] = prod[:, LANES:]
        for o, h in blocks:
            swap(o, h).start()

    swapped = set()

    def pair_sum(o, q):
        at = (o % NY, q // 2)
        if at not in swapped:
            swap(*at).wait_recv()
            swapped.add(at)
        mine = part[o % NY, core, part_of(q), :].astype(F32)
        return mine + sib[o % NY, part_of(q), :].astype(F32)

    def push(k, i):
        j = slots[k, i]
        return rcopy(tosend.at[j], arrived.at[j], rs_send, rs_recv.at[pair_index(k, i)], to_y(streams[k][1]))

    landed = set()

    def came(k, i):
        at = pair_index(k, i)
        if at not in landed:
            wait_bytes(arrived.at[pl.ds(0, 2)], rs_recv.at[at])
            landed.add(at)
        return arrived[slots[k, i]].astype(F32)

    def feed(k, i):
        q, s, n = streams[k]
        value = pair_sum(s * (n - i), q)
        if i:
            value = value + came(k, i - 1)
        tosend[slots[k, i]] = value.astype(BF16)
        push(k, i).start()

    def feed_all(p, i):
        for k in live(p, i):
            feed(k, i)

    def sides(i, h):
        m = reach - 1 - i
        return [] if m < 0 else [(o, h) for o in sorted({-m, m})]

    expand((reach, 0))
    activate(0)
    project((reach, 0))
    if far:
        expand((-far, 1))
    expand((reach, 1))
    activate(1)
    project((reach, 1))
    project(*sides(0, 1))
    feed_all(2, 0)
    feed_all(0, 0)
    project(*sides(0, 0))
    feed_all(3, 0)
    project(*sides(1, 1))
    feed_all(1, 0)
    for i in range(1, reach):
        for at, p in enumerate((2, 0, 3, 1)):
            feed_all(p, i)
            coming = ([], sides(i, 0), [], sides(i + 1, 1))[at]
            if coming:
                project(*coming)
            if (i, at) == (1, 2 if far > 1 else 0):
                prefix_part()
            elif later:
                later.pop(0)()
    for piece in later:
        piece()
    units = quarter // QUAD
    for h in (1, 0):
        for q in (2 * h, 2 * h + 1):
            value = pair_sum(0, q)
            for k in (2 * q, 2 * q + 1):
                if streams[k][2] > 0:
                    value = value + came(k, streams[k][2] - 1)
            put(rout.at[pl.ds(q * units, units)], value.astype(BF16))
        for offset, tgt in reaches:
            if seat[offset] // (EP // 2) == h:
                rcopy(
                    rout.at[pl.ds(seat[offset] * UC, UC)], rin.at[pl.ds(ep * UC, UC)], rt_send, rt_recv, at_ep(tgt)
                ).start()
    rin[pl.ds(ep * UC, UC)] = rout[pl.ds(0, UC)]

    final_part()
    wait_bytes(outbox.at[pl.ds(0, (EP - 1) * UC)], disp_send)
    halo_copy.wait_send()
    wait_bytes(sout.at[pl.ds(0, EP - 1)], st_send)
    wait_bytes(hout.at[pl.ds(0, EP - 1)], hb_send)
    wait_bytes(xall.at[pl.ds(0, NY - 1)], ag_send)
    wait_bytes(xall.at[pl.ds(0, NY)], d2_send)
    wait_bytes(sib, ps_send)
    wait_bytes(tosend, rs_send)

    wait_bytes(rout.at[pl.ds(0, (EP - 1) * UC)], rt_recv)
    back = flat(rin[...])
    moe_ref[...] = (mm(pick[0], back) + mm(pick[1], back)).astype(BF16)
    wait_bytes(rout.at[pl.ds(0, (EP - 1) * UC)], rt_send)


def place_body(mixed_ref, moe_ref, mixed_out, moe_out, sem):
    copies = [
        pltpu.make_async_copy(mixed_ref, mixed_out, sem.at[0]),
        pltpu.make_async_copy(moe_ref, moe_out, sem.at[1]),
    ]
    for copy in copies:
        copy.start()
    for copy in copies:
        copy.wait()


def on_device(EP, TP, *args):
    (x_in, z_in, dt_raw, decay_rate, b_in, c_in, conv_x, conv_b, conv_c, head_gain,
     moe_rows, moe_gain, routes, route_logit, w_gate, w_up, w_down) = args
    tokens, features = moe_rows.shape
    CAP = 2 * tokens * routes.shape[1] // EP
    VR, L = x_in.shape
    HH = dt_raw.shape[0]
    FD = w_gate.shape[2]
    flipped = functools.partial(jnp.swapaxes, axis1=-2, axis2=-1)
    NY = TP // 2
    ROWS = EP * CAP
    U = VR // EP
    UR = -(-(U + 8) // 16) * 16
    cfg = dict(EP=EP, TP=TP, CAP=CAP, L=L, HH=HH)
    hbm, vmem = (pl.BlockSpec(memory_space=m) for m in (pltpu.HBM, pltpu.VMEM))
    dma = pltpu.SemaphoreType.DMA
    units = (ROWS // QUAD, QUAD, LANES)
    block = (ROWS, LANES)
    piece = (ROWS // 4, LANES)
    hops = 4 * (2 * (NY // 2) - 1)
    scratch = [
        pltpu.VMEM((HH, L), F32), pltpu.VMEM((1, HH), F32),
        pltpu.VMEM((4, VR), F32), pltpu.VMEM((4, conv_b.shape[0]), F32), pltpu.VMEM((4, conv_b.shape[0]), F32),
        pltpu.VMEM((1, VR), F32), pltpu.VMEM((TP, features // TP), F32),
        pltpu.VMEM((2, tokens), jnp.int32), pltpu.VMEM((2, tokens), F32),
        pltpu.VMEM((VR, L), BF16), pltpu.VMEM((VR, L), BF16),
        pltpu.VMEM((NSTATE, L), BF16), pltpu.VMEM((NSTATE, L), BF16),
        pltpu.VMEM((tokens, features), BF16),
        pltpu.VMEM((FD, features), BF16), pltpu.VMEM((FD, features), BF16), pltpu.VMEM((FD, features), BF16),
        pltpu.VMEM((VR + 2 * NSTATE, LANES), BF16),
        pltpu.VMEM((16, VR + 2 * NSTATE), BF16), pltpu.VMEM((16, VR + 2 * NSTATE), BF16),
        pltpu.VMEM((2, tokens, ROWS), BF16),
        pltpu.VMEM(units, BF16), pltpu.VMEM(units, BF16), pltpu.VMEM((TP,) + block, BF16),
        pltpu.VMEM((ROWS, FD), F32), pltpu.VMEM((ROWS, FD), F32), pltpu.VMEM((ROWS, FD), BF16),
        pltpu.VMEM((NY, 2) + block, BF16), pltpu.VMEM((NY,) + block, BF16),
        pltpu.VMEM((hops,) + piece, BF16), pltpu.VMEM((hops,) + piece, BF16),
        pltpu.VMEM(units, BF16), pltpu.VMEM(units, BF16),
        pltpu.VMEM((VR, L), BF16), pltpu.VMEM((NSTATE, L), BF16), pltpu.VMEM((NSTATE, L), BF16),
        pltpu.VMEM((L, L), F32), pltpu.VMEM((8, L), F32), pltpu.VMEM((L, 8), F32), pltpu.VMEM((VR, L), F32),
        pltpu.VMEM((EP, UR, LANES), BF16), pltpu.VMEM((EP, UR, LANES), BF16),
        pltpu.VMEM((EP, U, LANES), F32), pltpu.VMEM((EP, U, LANES), F32),
        dma((17,)), dma, dma, dma, dma((2,)), dma, dma, dma, dma,
        dma, dma((hops // 2,)), dma, dma((NY, 2)), dma, dma((NY, 2)), dma, dma((hops // 2,)), dma, dma,
    ]
    mixed, moe = pl.pallas_call(
        functools.partial(kernel_body, cfg),
        name="mixer_and_experts",
        out_shape=(
            pltpu.VMEM((VR, L), BF16),
            pltpu.VMEM((tokens, features // TP), BF16),
        ),
        in_specs=[hbm] * 17,
        out_specs=(vmem, vmem),
        scratch_shapes=scratch,
        compiler_params=pltpu.CompilerParams(
            collective_id=0, has_side_effects=True, vmem_limit_bytes=60 * 1024 * 1024
        ),
    )(
        x_in, z_in, dt_raw, decay_rate.reshape(1, HH), b_in, c_in, flipped(conv_x), flipped(conv_b), flipped(conv_c),
        head_gain.reshape(1, VR), moe_rows, moe_gain.reshape(TP, features // TP),
        flipped(routes), flipped(route_logit), flipped(w_gate), flipped(w_up), w_down,
    )
    mixed, moe = pl.pallas_call(
        place_body,
        name="place",
        out_shape=(jax.ShapeDtypeStruct(mixed.shape, BF16), jax.ShapeDtypeStruct(moe.shape, BF16)),
        in_specs=[vmem, vmem],
        out_specs=(hbm, hbm),
        scratch_shapes=[dma((2,))],
    )(*(pltpu.with_memory_space_constraint(o, pltpu.VMEM) for o in (mixed, moe)))
    return mixed, flipped(moe)


def solution(mesh):
    EP, TP = mesh.shape["ep"], mesh.shape["tp"]
    in_specs = (
        P("tp", "ep"), P("tp", "ep"), P("tp", "ep"), P("tp"), P(None, "ep"), P(None, "ep"),
        P("tp", None), P(), P(), P("tp"), P("ep", None), P(), P("ep", None), P("ep", None),
        P("ep", None, "tp"), P("ep", None, "tp"), P("ep", "tp", None),
    )
    return jax.shard_map(
        functools.partial(on_device, EP, TP),
        mesh=mesh,
        in_specs=in_specs,
        out_specs=(P("tp", "ep"), P("tp", "ep")),
        check_vma=False,
    )
```
